32 devices in a mesh: kv: 16 (over z, y, x), tp: 2 (over core).
Axes of the slice: x: 2, y: 2, z: 4, core: 2. Of those that a mesh axis runs over, the one named last changes fastest.
Arguments:
- tokens: bfloat16 [64, 4, 2048], P('kv', None, 'tp'), may hold values from -6 to 6
- input_gain: float32 [2048], replicated, may hold values from 0.1 to 1.9
- gate_weight: bfloat16 [2048, 4096], P('kv', 'tp'), may hold values from -0.125 to 0.125
- value_weight: bfloat16 [2048, 4096], P('kv', 'tp'), may hold values from -0.125 to 0.125
- write_weight: bfloat16 [2048, 1024], P('kv', 'tp'), may hold values from -0.125 to 0.125
- read_weight: bfloat16 [2048, 1024], P('kv', 'tp'), may hold values from -0.125 to 0.125
- step_weight: bfloat16 [2048, 64], replicated, may hold values from -0.125 to 0.125
- conv_value: float32 [4, 4096], P(None, 'tp'), may hold values from -3 to 3
- conv_write: float32 [4, 1024], P(None, 'tp'), may hold values from -3 to 3
- conv_read: float32 [4, 1024], P(None, 'tp'), may hold values from -3 to 3
- step_bias: float32 [64], P('tp'), may hold values from -4 to -1
- decay_log: float32 [64], P('tp'), may hold values from 0 to 2.8
- skip_gain: float32 [64], P('tp'), may hold values from 0.5 to 1.5
- output_gain: float32 [4096], P('tp'), may hold values from 0.1 to 1.9
- out_weight: bfloat16 [4096, 2048], P('tp', 'kv'), may hold values from -0.09375 to 0.09375
- base_state: float32 [64, 64, 64, 128], P('kv', 'tp'), may hold values from -2 to 2
- past_value: bfloat16 [64, 7, 4096], P('kv', None, 'tp'), may hold values from -6 to 6
- past_write: bfloat16 [64, 7, 1024], P('kv', None, 'tp'), may hold values from -6 to 6
- past_read: bfloat16 [64, 7, 1024], P('kv', None, 'tp'), may hold values from -6 to 6
- past_step: bfloat16 [64, 4, 64], P('kv', None, 'tp'), may hold values from -4 to 4
- accepted: int32 [64], P('kv'), may hold values from 1 to 4
Outputs:
- mixed: bfloat16 [64, 4, 2048], P('kv', None, 'tp')
- root_state: float32 [64, 64, 64, 128], P('kv', 'tp')
- next_value: bfloat16 [64, 7, 4096], P('kv', None, 'tp')
- next_write: bfloat16 [64, 7, 1024], P('kv', None, 'tp')
- next_read: bfloat16 [64, 7, 1024], P('kv', None, 'tp')
- next_step: bfloat16 [64, 4, 64], P('kv', None, 'tp')
The draws below stay inside these ranges and needn't reach their ends.
Inputs may be any that keep to these rules, and one draw needn't show every extreme that they name: Every entry of `accepted` is an integer from 1 to 4 (at least one of the last step's proposals is always accepted).
All inputs are finite; a program needn't handle non-finite values.
Results may differ from the reference program's by a relative error of at most 0.018.
Values may be sent and summed in bfloat16 or wider, within the bound.
No kernel may reach another device: no remote copies, remote signals or barrier semaphores. Data moves between devices by JAX's collectives and lax.ppermute only.
A program may use at most 64 MiB of HBM per device.

```python
import jax
import jax.numpy as jnp
from jax import lax

WIDTH = 2048
INNER = 4096
HEADS = 64
HEAD_DIM = 64
GROUPS = 8
STATE_DIM = 128
CONV_W = 4
PROPOSALS = 4
SEQS = 64
PAST_ROWS = 7
N_TP = 2


def plant(entries, key, smallest, high):
    dims = entries.shape
    spot = [jax.random.randint(jax.random.fold_in(key, axis), (), 0, dims[axis]) for axis in range(len(dims))]
    entries = entries.at[tuple(spot)].set(smallest)
    longest = dims.index(max(dims))
    spot[longest] = (spot[longest] + 1) % dims[longest]
    return entries.at[tuple(spot)].set(high)


def levels(stream_key, shape, pieces, low, high):
    level = 1.0
    for dim, parts in pieces:
        draws = jax.random.uniform(jax.random.fold_in(jax.random.fold_in(stream_key, 6), dim), (parts,), jnp.float32, low / len(pieces), high / len(pieces))
        level = level * jnp.repeat(jnp.exp(draws), shape[dim] // parts).reshape((-1,) + (1,) * (len(shape) - 1 - dim))
    return level


def noise(key, extent, scale, most, shards=(), kind=jnp.bfloat16):
    loudness = levels(key, extent, shards, -0.22, 0.18) if shards else 1.0
    values = jax.random.normal(key, extent, jnp.float32) * scale * loudness
    return jnp.minimum(jnp.maximum(values, -most), most).astype(kind)


def setup_inputs(seed: int = 0) -> dict:
    key_of = jax.random.split(jax.random.key(seed), 22)
    tokens = noise(key_of[0], (SEQS, PROPOSALS, WIDTH), 1.0, 6.0, ((0, 16), (2, 2)))
    input_gain = jnp.clip(1.0 + 0.18 * jax.random.normal(key_of[1], (WIDTH,), jnp.float32), 0.1, 1.9)
    gate_weight = noise(key_of[2], (WIDTH, INNER), WIDTH ** -0.5, 0.125, ((0, 16), (1, 2)))
    value_weight = noise(key_of[3], (WIDTH, INNER), WIDTH ** -0.5, 0.125, ((0, 16), (1, 2)))
    write_weight = noise(key_of[4], (WIDTH, GROUPS * STATE_DIM), WIDTH ** -0.5, 0.125, ((0, 16), (1, 2)))
    read_weight = noise(key_of[5], (WIDTH, GROUPS * STATE_DIM), WIDTH ** -0.5, 0.125, ((0, 16), (1, 2)))
    step_weight = noise(key_of[6], (WIDTH, HEADS), WIDTH ** -0.5, 0.125)
    conv_value = noise(key_of[7], (CONV_W, INNER), 0.5, 3.0, ((1, 2),), jnp.float32)
    conv_write = noise(key_of[8], (CONV_W, GROUPS * STATE_DIM), 0.5, 3.0, ((1, 2),), jnp.float32)
    conv_read = noise(key_of[9], (CONV_W, GROUPS * STATE_DIM), 0.5, 3.0, ((1, 2),), jnp.float32)
    step_bias = jnp.clip(-4.0 + 3.0 * jax.random.uniform(key_of[10], (HEADS,), jnp.float32) ** levels(key_of[10], (HEADS,), ((0, 2),), -0.2, 0.2), -4.0, -1.0)
    decay_log = jnp.clip(2.8 * jax.random.uniform(key_of[11], (HEADS,), jnp.float32) ** levels(key_of[11], (HEADS,), ((0, 2),), -0.2, 0.2), 0.0, 2.8)
    skip_gain = jnp.clip(0.5 + 1.0 * jax.random.uniform(key_of[12], (HEADS,), jnp.float32) ** levels(key_of[12], (HEADS,), ((0, 2),), -0.2, 0.2), 0.5, 1.5)
    output_gain = jnp.clip(1.0 + 0.18 * jax.random.normal(key_of[13], (INNER,), jnp.float32), 0.1, 1.9)
    out_weight = noise(key_of[14], (INNER, WIDTH), INNER ** -0.5, 0.09375, ((0, 2), (1, 16)))
    base_state = noise(key_of[15], (SEQS, HEADS, HEAD_DIM, STATE_DIM), 0.3, 2.0, ((0, 16), (1, 2)), jnp.float32)
    past_value = noise(key_of[16], (SEQS, PAST_ROWS, INNER), 1.0, 6.0, ((0, 16), (2, 2)))
    past_write = noise(key_of[17], (SEQS, PAST_ROWS, GROUPS * STATE_DIM), 1.0, 6.0, ((0, 16), (2, 2)))
    past_read = noise(key_of[18], (SEQS, PAST_ROWS, GROUPS * STATE_DIM), 1.0, 6.0, ((0, 16), (2, 2)))
    past_step = noise(key_of[19], (SEQS, PROPOSALS, HEADS), 1.0, 4.0, ((0, 16), (2, 2)))
    accepted = plant(jax.random.randint(key_of[20], (SEQS,), 1, PROPOSALS + 1), jax.random.fold_in(key_of[20], 1), 1, PROPOSALS).astype(jnp.int32)
    return dict(tokens=tokens, input_gain=input_gain, gate_weight=gate_weight, value_weight=value_weight, write_weight=write_weight, read_weight=read_weight, step_weight=step_weight, conv_value=conv_value, conv_write=conv_write, conv_read=conv_read, step_bias=step_bias, decay_log=decay_log, skip_gain=skip_gain, output_gain=output_gain, out_weight=out_weight, base_state=base_state, past_value=past_value, past_write=past_write, past_read=past_read, past_step=past_step, accepted=accepted)


EPSILON = 1e-06

def causal_conv(rows, kernel):
    width = kernel.shape[0]
    count = rows.shape[0] - width + 1
    total = kernel[0] * rows[0:count]
    for offset in range(1, width):
        total = total + kernel[offset] * rows[offset:offset + count]
    return total

def advance(past_x, past_b, past_c, past_dt, taken, state_zero, value_now, write_now, read_now, gate_now, step_now, conv_value, conv_write, conv_read, step_bias, decay_log, skip_gain, output_gain):
    highest = lax.Precision.HIGHEST
    proposals = value_now.shape[0]
    head_count = step_bias.shape[0]
    group_count = write_now.shape[1] // STATE_DIM
    per_group = head_count // group_count
    head_width = value_now.shape[1] // head_count
    rate = jnp.exp(decay_log)
    taken = taken.astype(jnp.int32)
    prev_x = jax.nn.silu(causal_conv(past_x.astype(jnp.float32), conv_value)).reshape(proposals, head_count, head_width)
    prev_b = jax.nn.silu(causal_conv(past_b.astype(jnp.float32), conv_write)).reshape(proposals, group_count, STATE_DIM)
    prev_b = jnp.repeat(prev_b, per_group, axis=1)
    prev_dt = jax.nn.softplus(past_dt.astype(jnp.float32) + step_bias)
    live = (jnp.arange(proposals, dtype=jnp.int32) < taken)[:, None]
    prev_log = jnp.where(live, -rate * prev_dt, jnp.zeros_like(prev_dt))
    total_log = lax.optimization_barrier(jnp.sum(prev_log, axis=0))
    tail_log = total_log - jnp.cumsum(prev_log, axis=0)
    weight_now = jnp.where(live, jnp.exp(tail_log) * prev_dt, jnp.zeros_like(prev_dt))
    root = jnp.exp(total_log)[:, None, None] * state_zero + jnp.einsum('sh,shp,shn->hpn', weight_now, prev_x, prev_b, precision=highest)
    window_x = jnp.concatenate([lax.dynamic_slice_in_dim(past_x, taken, CONV_W - 1, 0), value_now], axis=0)
    window_b = jnp.concatenate([lax.dynamic_slice_in_dim(past_b, taken, CONV_W - 1, 0), write_now], axis=0)
    window_c = jnp.concatenate([lax.dynamic_slice_in_dim(past_c, taken, CONV_W - 1, 0), read_now], axis=0)
    cur_x = jax.nn.silu(causal_conv(window_x.astype(jnp.float32), conv_value)).reshape(proposals, head_count, head_width)
    cur_b = jax.nn.silu(causal_conv(window_b.astype(jnp.float32), conv_write)).reshape(proposals, group_count, STATE_DIM)
    cur_c = jax.nn.silu(causal_conv(window_c.astype(jnp.float32), conv_read)).reshape(proposals, group_count, STATE_DIM)
    cur_b = jnp.repeat(cur_b, per_group, axis=1)
    cur_c = jnp.repeat(cur_c, per_group, axis=1)
    cur_dt = jax.nn.softplus(step_now.astype(jnp.float32) + step_bias)
    logs = jnp.cumsum(-rate * cur_dt, axis=0)
    carried = jnp.einsum('thn,hpn->thp', cur_c, root, precision=highest) * jnp.exp(logs)[:, :, None]
    lower = (jnp.arange(proposals)[:, None] >= jnp.arange(proposals)[None, :])[:, :, None]
    diff = logs[:, None, :] - logs[None, :, :]
    decay = jnp.where(lower, jnp.exp(jnp.where(lower, diff, jnp.zeros_like(diff))), jnp.zeros_like(diff))
    scores = jnp.einsum('thn,shn->tsh', cur_c, cur_b, precision=highest) * decay * cur_dt[None, :, :]
    inner = jnp.einsum('tsh,shp->thp', scores, cur_x, precision=highest)
    mixed = carried + inner + skip_gain[None, :, None] * cur_x
    gated = mixed.reshape(proposals, -1) * jax.nn.silu(gate_now.astype(jnp.float32))
    grouped = gated.reshape(proposals, group_count, -1)
    grouped = grouped * lax.rsqrt(lax.optimization_barrier(jnp.mean(grouped * grouped, axis=-1, keepdims=True)) + EPSILON)
    result = (grouped.reshape(proposals, -1) * output_gain).astype(jnp.bfloat16)
    return (result, root, window_x, window_b, window_c)

def reference(tokens, input_gain, gate_weight, value_weight, write_weight, read_weight, step_weight, conv_value, conv_write, conv_read, step_bias, decay_log, skip_gain, output_gain, out_weight, base_state, past_value, past_write, past_read, past_step, accepted):
    seq_count, proposals, width = tokens.shape
    rows = tokens.astype(jnp.float32)
    normed = (rows * lax.rsqrt(lax.optimization_barrier(jnp.mean(rows * rows, axis=-1, keepdims=True)) + EPSILON) * input_gain).astype(jnp.bfloat16)
    flat = normed.reshape(seq_count * proposals, width)

    def project(weight):
        product = jnp.dot(flat, weight, preferred_element_type=jnp.float32).astype(jnp.bfloat16)
        return product.reshape(seq_count, proposals, weight.shape[1])
    gate_now = project(gate_weight)
    value_now = project(value_weight)
    write_now = project(write_weight)
    read_now = project(read_weight)
    step_now = project(step_weight)

    def one_sequence(items):
        return advance(*items, conv_value, conv_write, conv_read, step_bias, decay_log, skip_gain, output_gain)
    normal_out, root_state, next_value, next_write, next_read = lax.map(one_sequence, (past_value, past_write, past_read, past_step, accepted, base_state, value_now, write_now, read_now, gate_now, step_now))
    flat_y = normal_out.reshape(seq_count * proposals, -1)
    block = flat_y.shape[1] // N_TP
    total = jnp.zeros((seq_count * proposals, width), jnp.float32)
    for portion in range(N_TP):
        partial_sum = jnp.dot(flat_y[:, portion * block:(portion + 1) * block], out_weight[portion * block:(portion + 1) * block], preferred_element_type=jnp.float32)
        total = total + lax.optimization_barrier(partial_sum.astype(jnp.bfloat16)).astype(jnp.float32)
    mixed = total.astype(jnp.bfloat16).reshape(seq_count, proposals, width)
    return (mixed, root_state, next_value, next_write, next_read, step_now)
```

```python
import jax
import jax.numpy as jnp
from jax import lax
from jax.sharding import PartitionSpec as P

STATE_DIM = 128
CONV_W = 4
EPSILON = 1e-06


def causal_conv(rows, kernel):
    width = kernel.shape[0]
    count = rows.shape[0] - width + 1
    total = kernel[0] * rows[0:count]
    for offset in range(1, width):
        total = total + kernel[offset] * rows[offset : offset + count]
    return total


def advance(
    past_x,
    past_b,
    past_c,
    past_dt,
    taken,
    state_zero,
    value_now,
    write_now,
    read_now,
    gate_now,
    step_now,
    conv_value,
    conv_write,
    conv_read,
    step_bias,
    decay_log,
    skip_gain,
    output_gain,
):
    highest = lax.Precision.HIGHEST
    proposals = value_now.shape[0]
    head_count = step_bias.shape[0]
    group_count = write_now.shape[1] // STATE_DIM
    per_group = head_count // group_count
    head_width = value_now.shape[1] // head_count
    rate = jnp.exp(decay_log)
    prev_x = jax.nn.silu(causal_conv(past_x.astype(jnp.float32), conv_value)).reshape(
        proposals, head_count, head_width
    )
    prev_b = jax.nn.silu(causal_conv(past_b.astype(jnp.float32), conv_write)).reshape(
        proposals, group_count, STATE_DIM
    )
    prev_b = jnp.repeat(prev_b, per_group, axis=1)
    prev_dt = jax.nn.softplus(past_dt.astype(jnp.float32) + step_bias)
    live = (jnp.arange(proposals, dtype=jnp.int32) < taken)[:, None]
    prev_log = jnp.where(live, -rate * prev_dt, jnp.zeros_like(prev_dt))
    total_log = jnp.sum(prev_log, axis=0)
    tail_log = total_log - jnp.cumsum(prev_log, axis=0)
    weight_now = jnp.where(live, jnp.exp(tail_log) * prev_dt, jnp.zeros_like(prev_dt))
    root = jnp.exp(total_log)[:, None, None] * state_zero + jnp.einsum(
        "sh,shp,shn->hpn", weight_now, prev_x, prev_b, precision=highest
    )
    window_x = jnp.concatenate(
        [lax.dynamic_slice_in_dim(past_x, taken, CONV_W - 1, 0), value_now], axis=0
    )
    window_b = jnp.concatenate(
        [lax.dynamic_slice_in_dim(past_b, taken, CONV_W - 1, 0), write_now], axis=0
    )
    window_c = jnp.concatenate(
        [lax.dynamic_slice_in_dim(past_c, taken, CONV_W - 1, 0), read_now], axis=0
    )
    cur_x = jax.nn.silu(causal_conv(window_x.astype(jnp.float32), conv_value)).reshape(
        proposals, head_count, head_width
    )
    cur_b = jax.nn.silu(causal_conv(window_b.astype(jnp.float32), conv_write)).reshape(
        proposals, group_count, STATE_DIM
    )
    cur_c = jax.nn.silu(causal_conv(window_c.astype(jnp.float32), conv_read)).reshape(
        proposals, group_count, STATE_DIM
    )
    cur_b = jnp.repeat(cur_b, per_group, axis=1)
    cur_c = jnp.repeat(cur_c, per_group, axis=1)
    cur_dt = jax.nn.softplus(step_now.astype(jnp.float32) + step_bias)
    logs = jnp.cumsum(-rate * cur_dt, axis=0)
    carried = jnp.einsum("thn,hpn->thp", cur_c, root, precision=highest) * jnp.exp(logs)[:, :, None]
    lower = (jnp.arange(proposals)[:, None] >= jnp.arange(proposals)[None, :])[:, :, None]
    diff = logs[:, None, :] - logs[None, :, :]
    decay = jnp.where(
        lower, jnp.exp(jnp.where(lower, diff, jnp.zeros_like(diff))), jnp.zeros_like(diff)
    )
    scores = (
        jnp.einsum("thn,shn->tsh", cur_c, cur_b, precision=highest) * decay * cur_dt[None, :, :]
    )
    inner = jnp.einsum("tsh,shp->thp", scores, cur_x, precision=highest)
    mixed = carried + inner + skip_gain[None, :, None] * cur_x
    gated = mixed.reshape(proposals, -1) * jax.nn.silu(gate_now.astype(jnp.float32))
    grouped = gated.reshape(proposals, group_count, -1)
    grouped = grouped * lax.rsqrt(jnp.mean(grouped * grouped, axis=-1, keepdims=True) + EPSILON)
    result = (grouped.reshape(proposals, -1) * output_gain).astype(jnp.bfloat16)
    return (result, root, window_x, window_b, window_c)


def inner_size(ranks):
    size = 1
    while ranks % (2 * size) == 0 and 4 * size * size <= ranks:
        size = 2 * size
    return size


def swap(item, step):
    ranks = lax.axis_size("kv")
    return lax.ppermute(item, "kv", [(k, k ^ step) for k in range(ranks)])


def on_device(
    tokens,
    input_gain,
    gate_weight,
    value_weight,
    write_weight,
    read_weight,
    step_weight,
    conv_value,
    conv_write,
    conv_read,
    step_bias,
    decay_log,
    skip_gain,
    output_gain,
    out_weight,
    base_state,
    past_value,
    past_write,
    past_read,
    past_step,
    accepted,
):
    ranks = lax.axis_size("kv")
    halves = lax.axis_size("tp")
    me = lax.axis_index("kv")
    side = lax.axis_index("tp")
    inner = inner_size(ranks)
    outer = ranks // inner
    me_inner = lax.rem(me, inner)
    me_outer = lax.div(me, inner)

    weights = (gate_weight, value_weight, write_weight, read_weight)
    spans = [item.shape[1] // inner for item in weights]

    def piece(step):
        target = me_inner ^ step
        return jnp.concatenate(
            [
                lax.dynamic_slice_in_dim(item, target * span, span, 1)
                for item, span in zip(weights, spans)
            ],
            axis=1,
        )

    narrow = [piece(0)] + [swap(piece(step), step) for step in range(1, inner)]

    whole = lax.all_gather(tokens, "tp", axis=2, tiled=True)
    seq_local, proposals, width = whole.shape
    rows = whole.astype(jnp.float32)
    normed = (
        rows * lax.rsqrt(jnp.mean(rows * rows, axis=-1, keepdims=True) + EPSILON) * input_gain
    ).astype(jnp.bfloat16)
    flat = normed.reshape(seq_local * proposals, width)
    token_count = flat.shape[0]
    head_count = step_bias.shape[0]
    own_step = lax.dynamic_slice_in_dim(step_weight, side * head_count, head_count, 1)
    step_now = jnp.dot(flat, own_step, preferred_element_type=jnp.float32).astype(jnp.bfloat16)

    part = width // (outer * halves)
    share = lax.dynamic_index_in_dim(
        flat.reshape(token_count, outer, halves, part), side, 2, keepdims=False
    )
    share = jnp.broadcast_to(
        jnp.swapaxes(share, 0, 1)[:, None], (outer, inner, token_count, part)
    ).reshape(ranks * token_count, part)
    everyone = lax.all_to_all(share, "kv", split_axis=0, concat_axis=0, tiled=True)
    everyone = lax.all_gather(everyone, "tp", axis=1, tiled=True)

    block = width // ranks
    product = None
    for step in range(inner):
        term = jnp.dot(
            lax.dynamic_slice_in_dim(everyone, (me_inner ^ step) * block, block, 1),
            narrow[step],
            preferred_element_type=jnp.float32,
        )
        product = term if product is None else product + term
    returned = lax.all_to_all(
        product.astype(jnp.bfloat16), "kv", split_axis=0, concat_axis=0, tiled=True
    )
    returned = jnp.sum(
        returned.reshape(outer, inner, token_count, sum(spans)).astype(jnp.float32), axis=0
    ).astype(jnp.bfloat16)
    pieces_out = []
    offset = 0
    for span in spans:
        pieces_out.append(
            jnp.swapaxes(returned[:, :, offset : offset + span], 0, 1).reshape(
                token_count, inner * span
            )
        )
        offset = offset + span
    gate_now, value_now, write_now, read_now = pieces_out

    columns = [out_weight] + [swap(out_weight, step) for step in range(1, inner)]

    shaped = [
        item.reshape(seq_local, proposals, item.shape[1])
        for item in (value_now, write_now, read_now, gate_now, step_now)
    ]
    stepper = jax.vmap(advance, in_axes=(0,) * 11 + (None,) * 7)
    normal_out, root_state, next_value, next_write, next_read = stepper(
        past_value,
        past_write,
        past_read,
        past_step,
        accepted,
        base_state,
        shaped[0],
        shaped[1],
        shaped[2],
        shaped[3],
        shaped[4],
        conv_value,
        conv_write,
        conv_read,
        step_bias,
        decay_log,
        skip_gain,
        output_gain,
    )
    flat_y = normal_out.reshape(token_count, -1)
    stacked = jnp.concatenate(
        [flat_y] + [swap(flat_y, inner * step) for step in range(1, outer)], axis=0
    )
    partial = jnp.concatenate(
        [
            jnp.dot(stacked, item, preferred_element_type=jnp.float32).astype(jnp.bfloat16)
            for item in columns
        ],
        axis=1,
    ).reshape(outer, token_count, -1)
    blocks = jnp.stack(
        [partial[0]] + [swap(partial[step], inner * step) for step in range(1, outer)]
    ).reshape(outer, token_count, inner, -1)
    order_outer = me_outer ^ jnp.arange(outer)
    order_inner = me_inner ^ jnp.arange(inner)
    blocks = jnp.take(jnp.take(blocks, order_outer, axis=0), order_inner, axis=2)
    full = jnp.swapaxes(blocks, 0, 1).reshape(token_count, halves, width // halves)
    shares = lax.all_to_all(full, "tp", split_axis=1, concat_axis=1, tiled=True)
    mixed = jnp.sum(shares.astype(jnp.float32), axis=1).astype(jnp.bfloat16)
    mixed = mixed.reshape(seq_local, proposals, width // halves)
    return (mixed, root_state, next_value, next_write, next_read, shaped[4])


def solution(mesh):
    return jax.shard_map(
        on_device,
        mesh=mesh,
        in_specs=(
            P("kv", None, "tp"),
            P(),
            P("kv", "tp"),
            P("kv", "tp"),
            P("kv", "tp"),
            P("kv", "tp"),
            P(),
            P(None, "tp"),
            P(None, "tp"),
            P(None, "tp"),
            P("tp"),
            P("tp"),
            P("tp"),
            P("tp"),
            P("tp", "kv"),
            P("kv", "tp", None, None),
            P("kv", None, "tp"),
            P("kv", None, "tp"),
            P("kv", None, "tp"),
            P("kv", None, "tp"),
            P("kv"),
        ),
        out_specs=(
            P("kv", None, "tp"),
            P("kv", "tp", None, None),
            P("kv", None, "tp"),
            P("kv", None, "tp"),
            P("kv", None, "tp"),
            P("kv", None, "tp"),
        ),
        check_vma=False,
    )
```

```python
import functools

import jax
import jax.numpy as jnp
from jax import lax
from jax.experimental import pallas as pl
from jax.experimental.pallas import tpu as pltpu
from jax.sharding import PartitionSpec as P

STATE_DIM = 128
CONV_W = 4
EPSILON = 1e-06


def silu(v):
    return v / (1.0 + jnp.exp(-v))


def softplus(v):
    return jnp.maximum(v, 0.0) + jnp.log1p(jnp.exp(-jnp.abs(v)))


def spread(heads, width):
    lane = lax.broadcasted_iota(jnp.int32, (heads, heads * width), 1)
    head = lax.broadcasted_iota(jnp.int32, (heads, heads * width), 0)
    return jnp.where(lane // width == head, 1.0, 0.0)


def halves_of(item):
    high = item.astype(jnp.bfloat16).astype(jnp.float32)
    return high, item - high


def root_kernel(
    taken_ref,
    base_ref,
    past_x_ref,
    past_b_ref,
    past_dt_ref,
    conv_x_ref,
    conv_b_ref,
    bias_ref,
    decay_ref,
    root_ref,
    short_ref,
):
    _, heads, width, states = base_ref.shape
    steps = past_dt_ref.shape[1]
    groups = past_b_ref.shape[2] // states
    span = heads * width // groups
    taken = taken_ref[pl.program_id(0)]
    copies = spread(heads, width)
    fixed = jnp.dot(
        jnp.concatenate([bias_ref[...], decay_ref[...]], axis=0),
        copies,
        precision=lax.Precision.HIGHEST,
        preferred_element_type=jnp.float32,
    )
    step = jnp.dot(
        past_dt_ref[0], copies.astype(jnp.bfloat16), preferred_element_type=jnp.float32
    )
    dt = softplus(step + fixed[0:1])
    live = lax.broadcasted_iota(jnp.int32, dt.shape, 0) < taken
    logs = jnp.where(live, -jnp.exp(fixed[1:2]) * dt, 0.0)
    tails = [jnp.zeros_like(logs[0:1])]
    for row in range(steps - 1, 0, -1):
        tails.insert(0, tails[0] + logs[row : row + 1])
    total = tails[0] + logs[0:1]
    weight = jnp.where(live, jnp.exp(jnp.concatenate(tails, axis=0)) * dt, 0.0)

    def conv(rows, taps):
        return sum(taps[k : k + 1] * rows[k : k + steps] for k in range(CONV_W))

    left = weight * silu(conv(past_x_ref[0].astype(jnp.float32), conv_x_ref[...]))
    right = silu(conv(past_b_ref[0].astype(jnp.float32), conv_b_ref[...]))
    left_high, left_low = halves_of(left)
    right_high, right_low = halves_of(right)
    scale = jnp.exp(total)
    scale_high, rest = halves_of(scale)
    scale_mid, rest = halves_of(rest)
    lhs = jnp.concatenate(
        [left_high, left_high, left_low, scale_high, scale_mid, rest, jnp.zeros_like(rest)], axis=0
    ).astype(jnp.bfloat16)
    rhs = jnp.concatenate([right_high, right_low, right_high], axis=0)
    rhs = jnp.concatenate([rhs, jnp.zeros((4, rhs.shape[1]), jnp.float32)], axis=0).astype(
        jnp.bfloat16
    )
    row = lax.broadcasted_iota(jnp.int32, (3 * steps + 4, states), 0)
    ones = jnp.where((row >= 3 * steps) & (row < 3 * steps + 3), 1.0, 0.0).astype(jnp.bfloat16)
    each = heads // groups
    for group in range(groups):
        both = lax.dot_general(
            lhs[:, group * span : (group + 1) * span],
            jnp.concatenate([rhs[:, group * states : (group + 1) * states], ones], axis=1),
            (((0,), (0,)), ((), ())),
            preferred_element_type=jnp.float32,
        )
        base = base_ref[0, group * each : (group + 1) * each].reshape(span, states)
        root = both[:, states:] * base + both[:, :states]
        root_ref[0, group * each : (group + 1) * each] = root.reshape(each, width, states)
        short_ref[0, group * span : (group + 1) * span] = root.astype(jnp.bfloat16)


def make_root(base, past_x, past_b, past_dt, taken, conv_x, conv_b, bias, decay):
    count, heads, width, states = base.shape

    def one(*dims):
        return pl.BlockSpec((1,) + dims, lambda s: (s,) + (0,) * len(dims))

    def same(item):
        return pl.BlockSpec(item.shape, lambda s: (0,) * item.ndim)

    args = (past_x, past_b, past_dt)
    fixed = (conv_x, conv_b, bias[None], decay[None])
    return pl.pallas_call(
        root_kernel,
        grid=(count,),
        in_specs=[pl.BlockSpec(memory_space=pltpu.SMEM), one(*base.shape[1:])]
        + [one(*item.shape[1:]) for item in args]
        + [same(item) for item in fixed],
        out_specs=[one(*base.shape[1:]), one(heads * width, states)],
        out_shape=[
            jax.ShapeDtypeStruct(base.shape, jnp.float32),
            jax.ShapeDtypeStruct((count, heads * width, states), jnp.bfloat16),
        ],
        cost_estimate=pl.CostEstimate(
            flops=4 * base.size * 16, bytes_accessed=10 * base.size, transcendentals=0
        ),
        name="root",
    )(taken, base, *args, *fixed)


def mixer_kernel(
    outer,
    inner,
    spans,
    taken_ref,
    parts_ref,
    short_ref,
    step_ref,
    past_x_ref,
    past_b_ref,
    past_c_ref,
    conv_x_ref,
    conv_b_ref,
    conv_c_ref,
    bias_ref,
    decay_ref,
    skip_ref,
    gain_ref,
    out_ref,
    next_x_ref,
    next_b_ref,
    next_c_ref,
    now_ref,
):
    count, kept, channels = past_x_ref.shape
    tokens = step_ref.shape[0]
    steps = tokens // count
    heads = bias_ref.shape[1]
    states = short_ref.shape[2]
    groups = past_b_ref.shape[2] // states
    span = channels // groups
    starts = (0, channels, 2 * channels, 2 * channels + groups * states)

    for block in range(inner):
        for kind in range(4):
            low = sum(spans[:kind])
            total = None
            for shard in range(outer):
                term = parts_ref[shard * inner + block, :, low : low + spans[kind]].astype(
                    jnp.float32
                )
                total = term if total is None else total + term
            first = starts[kind] + block * spans[kind]
            now_ref[:, first : first + spans[kind]] = total.astype(jnp.bfloat16)

    stride = kept + 1

    def pick(rows, source_of, columns):
        row = lax.broadcasted_iota(jnp.int32, (rows, columns), 0)
        column = lax.broadcasted_iota(jnp.int32, (rows, columns), 1)
        return source_of(row, column)

    def from_past(row, column):
        found = jnp.zeros(row.shape, jnp.bool_)
        for s in range(count):
            place, seq = window_place(row)
            hit = (seq == s) & (place < CONV_W - 1)
            found = found | (hit & (column == s * stride + taken_ref[s] + place))
        return jnp.where(found, 1.0, 0.0).astype(jnp.bfloat16)

    def from_now(row, column):
        place, seq = window_place(row)
        hit = (place >= CONV_W - 1) & (place < kept)
        hit = hit & (column == seq * steps + place - (CONV_W - 1))
        return jnp.where(hit, 1.0, 0.0).astype(jnp.bfloat16)

    def window_place(row):
        tap, token = row // tokens, row % tokens
        other = row - CONV_W * tokens
        is_tap = row < CONV_W * tokens
        place = jnp.where(is_tap, tap + token % steps, other % stride)
        seq = jnp.where(is_tap, token // steps, other // stride)
        return place, seq

    rows = CONV_W * tokens + count * stride
    pick_past = pick(rows, from_past, count * stride)
    pick_now = pick(rows, from_now, tokens)

    def window(past_ref, first, taps_ref, next_ref):
        size = past_ref.shape[2]
        past = jnp.concatenate(
            [
                jnp.concatenate(
                    [past_ref[s].astype(jnp.float32), jnp.zeros((1, size), jnp.float32)], axis=0
                )
                for s in range(count)
            ],
            axis=0,
        ).astype(jnp.bfloat16)
        picked = jnp.dot(pick_past, past, preferred_element_type=jnp.float32) + jnp.dot(
            pick_now, now_ref[:, first : first + size], preferred_element_type=jnp.float32
        )
        for s in range(count):
            low = CONV_W * tokens + s * stride
            next_ref[s] = picked[low : low + kept].astype(jnp.bfloat16)
        return silu(
            sum(
                taps_ref[k : k + 1] * picked[k * tokens : (k + 1) * tokens] for k in range(CONV_W)
            )
        )

    x = window(past_x_ref, starts[1], conv_x_ref, next_x_ref)
    b = window(past_b_ref, starts[2], conv_b_ref, next_b_ref)
    c = window(past_c_ref, starts[3], conv_c_ref, next_c_ref)

    copies = spread(heads, channels // heads)
    fixed = jnp.dot(
        jnp.concatenate([bias_ref[...], decay_ref[...], skip_ref[...]], axis=0),
        copies,
        precision=lax.Precision.HIGHEST,
        preferred_element_type=jnp.float32,
    )
    dt = softplus(
        jnp.dot(step_ref[...], copies.astype(jnp.bfloat16), preferred_element_type=jnp.float32)
        + fixed[0:1]
    )
    one = -jnp.exp(fixed[1:2]) * dt
    place = lax.broadcasted_iota(jnp.int32, (tokens, 1), 0) % steps
    seq = lax.broadcasted_iota(jnp.int32, (tokens, 1), 0) // steps
    logs = one
    for back in range(1, steps):
        logs = logs + jnp.where(place >= back, pltpu.roll(one, back, 0), 0.0)

    c_short = c.astype(jnp.bfloat16)
    carried = []
    for group in range(groups):
        total = None
        for s in range(count):
            term = lax.dot_general(
                c_short[:, group * states : (group + 1) * states],
                short_ref[s, group * span : (group + 1) * span],
                (((1,), (1,)), ((), ())),
                preferred_element_type=jnp.float32,
            )
            total = term if total is None else jnp.where(seq == s, term, total)
        carried.append(total)
    y = jnp.exp(logs) * jnp.concatenate(carried, axis=1) + fixed[2:3] * x
    for back in range(steps):
        other_b = pltpu.roll(b, back, 0) if back else b
        score = jnp.concatenate(
            [
                jnp.broadcast_to(
                    jnp.sum(
                        (c * other_b)[:, g * states : (g + 1) * states], axis=1, keepdims=True
                    ),
                    (tokens, span),
                )
                for g in range(groups)
            ],
            axis=1,
        )
        if back:
            drop = jnp.where(place >= back, logs - pltpu.roll(logs, back, 0), 0.0)
            term = jnp.exp(drop) * score * pltpu.roll(dt * x, back, 0)
            y = y + jnp.where(place >= back, term, 0.0)
        else:
            y = y + score * (dt * x)
    g = y * silu(now_ref[:, 0:channels].astype(jnp.float32))
    for group in range(groups):
        cols = slice(group * span, (group + 1) * span)
        part = g[:, cols]
        mean = jnp.sum(part * part, axis=1, keepdims=True) * (1.0 / span)
        out_ref[:, cols] = (part * lax.rsqrt(mean + EPSILON) * gain_ref[:, cols]).astype(
            jnp.bfloat16
        )


def make_mixer(outer, inner, spans, taken, parts, short, step, pasts, convs, vectors):
    tokens = step.shape[0]
    args = (parts, short, step) + pasts + convs + tuple(item[None] for item in vectors)
    channels = pasts[0].shape[2]
    vmem = pl.BlockSpec(memory_space=pltpu.VMEM)
    return pl.pallas_call(
        functools.partial(mixer_kernel, outer, inner, spans),
        in_specs=[pl.BlockSpec(memory_space=pltpu.SMEM)] + [vmem] * len(args),
        out_specs=[vmem] * 4,
        out_shape=[jax.ShapeDtypeStruct((tokens, channels), jnp.bfloat16)]
        + [jax.ShapeDtypeStruct(item.shape, jnp.bfloat16) for item in pasts],
        scratch_shapes=[
            pltpu.VMEM((tokens, sum(item.shape[2] for item in pasts) + channels), jnp.bfloat16)
        ],
        cost_estimate=pl.CostEstimate(
            flops=4 * short.size * tokens, bytes_accessed=2 * short.size, transcendentals=0
        ),
        name="mixer",
    )(taken, *args)


def product_kernel(outer, inner, *refs):
    ys, columns, outs = refs[:outer], refs[outer : outer + inner], refs[outer + inner :]
    tokens = ys[0].shape[0]
    stacked = jnp.concatenate([item[...] for item in ys], axis=0)
    size = columns[0].shape[1]
    for step in range(inner):
        result = jnp.dot(stacked, columns[step][...], preferred_element_type=jnp.float32)
        result = result.astype(jnp.bfloat16)
        for shard in range(outer):
            outs[shard][:, step * size : (step + 1) * size] = result[
                shard * tokens : (shard + 1) * tokens
            ]


def make_product(ys, columns):
    outer, inner = len(ys), len(columns)
    tokens, depth = ys[0].shape
    size = columns[0].shape[1]
    vmem = pl.BlockSpec(memory_space=pltpu.VMEM)
    return pl.pallas_call(
        functools.partial(product_kernel, outer, inner),
        in_specs=[vmem] * (outer + inner),
        out_specs=[vmem] * outer,
        out_shape=[jax.ShapeDtypeStruct((tokens, inner * size), jnp.bfloat16)] * outer,
        cost_estimate=pl.CostEstimate(
            flops=2 * outer * tokens * depth * inner * size,
            bytes_accessed=2 * depth * inner * size,
            transcendentals=0,
        ),
        name="product",
    )(*ys, *columns)


def arrange_kernel(outer, inner, where_ref, *refs):
    keep_ref, send_ref = refs[outer:]
    size = refs[0].shape[1] // inner
    for step in range(outer):
        shard = where_ref[0] ^ step
        mine = lax.div(shard, outer // 2) == where_ref[2]
        for sub in range(inner):
            column = (lax.rem(shard, outer // 2) * inner + (where_ref[1] ^ sub)) * size
            column = pl.multiple_of(column, size)
            item = refs[step][:, sub * size : (sub + 1) * size]

            @pl.when(mine)
            def _(item=item, column=column):
                keep_ref[:, pl.ds(column, size)] = item

            @pl.when(jnp.logical_not(mine))
            def _(item=item, column=column):
                send_ref[:, pl.ds(column, size)] = item


def make_arranged(where, items, inner):
    outer = len(items)
    tokens, columns = items[0].shape
    vmem = pl.BlockSpec(memory_space=pltpu.VMEM)
    return pl.pallas_call(
        functools.partial(arrange_kernel, outer, inner),
        in_specs=[pl.BlockSpec(memory_space=pltpu.SMEM)] + [vmem] * outer,
        out_specs=[vmem] * 2,
        out_shape=[jax.ShapeDtypeStruct((tokens, outer // 2 * columns), jnp.bfloat16)] * 2,
        name="arrange",
    )(where, *items)


def join_kernel(left_ref, right_ref, out_ref):
    total = left_ref[...].astype(jnp.float32) + right_ref[...].astype(jnp.float32)
    steps = out_ref.shape[1]
    for s in range(out_ref.shape[0]):
        out_ref[s] = total[s * steps : (s + 1) * steps].astype(jnp.bfloat16)


def make_joined(left, right, count):
    tokens, columns = left.shape
    vmem = pl.BlockSpec(memory_space=pltpu.VMEM)
    return pl.pallas_call(
        join_kernel,
        in_specs=[vmem] * 2,
        out_specs=vmem,
        out_shape=jax.ShapeDtypeStruct((count, tokens // count, columns), jnp.bfloat16),
        name="join",
    )(left, right)


def inner_size(ranks):
    size = 1
    while ranks % (2 * size) == 0 and 4 * size * size <= ranks:
        size = 2 * size
    return size


def swap(item, step):
    ranks = lax.axis_size("kv")
    return lax.ppermute(item, "kv", [(k, k ^ step) for k in range(ranks)])


def on_device(
    tokens,
    input_gain,
    gate_weight,
    value_weight,
    write_weight,
    read_weight,
    step_weight,
    conv_value,
    conv_write,
    conv_read,
    step_bias,
    decay_log,
    skip_gain,
    output_gain,
    out_weight,
    base_state,
    past_value,
    past_write,
    past_read,
    past_step,
    accepted,
):
    ranks = lax.axis_size("kv")
    halves = lax.axis_size("tp")
    me = lax.axis_index("kv")
    side = lax.axis_index("tp")
    inner = inner_size(ranks)
    outer = ranks // inner
    me_inner = lax.rem(me, inner)
    me_outer = lax.div(me, inner)

    weights = (gate_weight, value_weight, write_weight, read_weight)
    spans = [item.shape[1] // inner for item in weights]

    def piece(step):
        target = me_inner ^ step
        return jnp.concatenate(
            [
                lax.dynamic_slice_in_dim(item, target * span, span, 1)
                for item, span in zip(weights, spans)
            ],
            axis=1,
        )

    narrow = [piece(0)] + [swap(piece(step), step) for step in range(1, inner)]

    whole = lax.all_gather(tokens, "tp", axis=2, tiled=True)
    seq_local, proposals, width = whole.shape
    rows = whole.astype(jnp.float32)
    normed = (
        rows * lax.rsqrt(jnp.mean(rows * rows, axis=-1, keepdims=True) + EPSILON) * input_gain
    ).astype(jnp.bfloat16)
    flat = normed.reshape(seq_local * proposals, width)
    token_count = flat.shape[0]
    head_count = step_bias.shape[0]
    own_step = lax.dynamic_slice_in_dim(step_weight, side * head_count, head_count, 1)
    step_now = jnp.dot(flat, own_step, preferred_element_type=jnp.float32).astype(jnp.bfloat16)

    part = width // (outer * halves)
    share = lax.dynamic_index_in_dim(
        flat.reshape(token_count, outer, halves, part), side, 2, keepdims=False
    )
    share = jnp.broadcast_to(
        jnp.swapaxes(share, 0, 1)[:, None], (outer, inner, token_count, part)
    ).reshape(ranks * token_count, part)
    everyone = lax.all_to_all(share, "kv", split_axis=0, concat_axis=0, tiled=True)
    everyone = lax.all_gather(everyone, "tp", axis=1, tiled=True)

    block = width // ranks
    product = None
    for step in range(inner):
        term = jnp.dot(
            lax.dynamic_slice_in_dim(everyone, (me_inner ^ step) * block, block, 1),
            narrow[step],
            preferred_element_type=jnp.float32,
        )
        product = term if product is None else product + term
    product = product.astype(jnp.bfloat16)
    out_weight, product = lax.optimization_barrier((out_weight, product))
    returned = lax.all_to_all(product, "kv", split_axis=0, concat_axis=0, tiled=True)
    columns = [out_weight] + [swap(out_weight, step) for step in range(1, inner)]
    returned = returned.reshape(ranks, token_count, sum(spans))
    shards, pieces = outer, inner
    if any(span % 128 for span in spans):
        summed = jnp.sum(
            returned.reshape(outer, inner, token_count, sum(spans)).astype(jnp.float32), axis=0
        ).astype(jnp.bfloat16)
        joined, offset = [], 0
        for span in spans:
            item = jnp.swapaxes(summed[:, :, offset : offset + span], 0, 1)
            joined.append(item.reshape(token_count, inner * span))
            offset = offset + span
        returned = jnp.concatenate(joined, axis=1)[None]
        spans = [inner * span for span in spans]
        shards, pieces = 1, 1

    root_state, short = make_root(
        base_state,
        past_value,
        past_write,
        past_step,
        accepted,
        conv_value,
        conv_write,
        step_bias,
        decay_log,
    )
    flat_y, next_value, next_write, next_read = make_mixer(
        shards,
        pieces,
        tuple(spans),
        accepted,
        returned,
        short,
        step_now,
        (past_value, past_write, past_read),
        (conv_value, conv_write, conv_read),
        (step_bias, decay_log, skip_gain, output_gain),
    )
    ys = [flat_y] + [swap(flat_y, inner * step) for step in range(1, outer)]
    step_out = step_now.reshape(seq_local, proposals, head_count)
    if out_weight.shape[1] % 128 == 0 and halves == 2:
        partial = make_product(ys, columns)
        blocks = [partial[0]] + [swap(partial[step], inner * step) for step in range(1, outer)]
        where = jnp.stack([me_outer, me_inner, side])
        keep, send = make_arranged(where, blocks, inner)
        other = lax.ppermute(send, "tp", [(0, 1), (1, 0)])
        mixed = make_joined(keep, other, seq_local)
        return (mixed, root_state, next_value, next_write, next_read, step_out)
    stacked = jnp.concatenate(ys, axis=0)
    partial = jnp.concatenate(
        [
            jnp.dot(stacked, item, preferred_element_type=jnp.float32).astype(jnp.bfloat16)
            for item in columns
        ],
        axis=1,
    ).reshape(outer, token_count, -1)
    blocks = jnp.stack(
        [partial[0]] + [swap(partial[step], inner * step) for step in range(1, outer)]
    ).reshape(outer, token_count, inner, -1)
    order_outer = me_outer ^ jnp.arange(outer)
    order_inner = me_inner ^ jnp.arange(inner)
    blocks = jnp.take(jnp.take(blocks, order_outer, axis=0), order_inner, axis=2)
    full = jnp.swapaxes(blocks, 0, 1).reshape(token_count, halves, width // halves)
    shares = lax.all_to_all(full, "tp", split_axis=1, concat_axis=1, tiled=True)
    mixed = jnp.sum(shares.astype(jnp.float32), axis=1).astype(jnp.bfloat16)
    mixed = mixed.reshape(seq_local, proposals, width // halves)
    return (mixed, root_state, next_value, next_write, next_read, step_out)


def solution(mesh):
    return jax.shard_map(
        on_device,
        mesh=mesh,
        in_specs=(
            P("kv", None, "tp"),
            P(),
            P("kv", "tp"),
            P("kv", "tp"),
            P("kv", "tp"),
            P("kv", "tp"),
            P(),
            P(None, "tp"),
            P(None, "tp"),
            P(None, "tp"),
            P("tp"),
            P("tp"),
            P("tp"),
            P("tp"),
            P("tp", "kv"),
            P("kv", "tp", None, None),
            P("kv", None, "tp"),
            P("kv", None, "tp"),
            P("kv", None, "tp"),
            P("kv", None, "tp"),
            P("kv"),
        ),
        out_specs=(
            P("kv", None, "tp"),
            P("kv", "tp", None, None),
            P("kv", None, "tp"),
            P("kv", None, "tp"),
            P("kv", None, "tp"),
            P("kv", None, "tp"),
        ),
        check_vma=False,
    )
```

```python
import functools

import jax
import jax.numpy as jnp
from jax import lax
from jax.experimental import pallas as pl
from jax.experimental.pallas import tpu as pltpu
from jax.sharding import PartitionSpec as P


CONV_W = 4
EPSILON = 1e-06


def silu(v):
    return v / (1.0 + jnp.exp(-v))


def softplus(v):
    return jnp.maximum(v, 0.0) + jnp.log1p(jnp.exp(-jnp.abs(v)))


def spread(heads, width):
    lane = lax.broadcasted_iota(jnp.int32, (heads, heads * width), 1)
    head = lax.broadcasted_iota(jnp.int32, (heads, heads * width), 0)
    return jnp.where(lane // width == head, 1.0, 0.0)


def halves_of(item):
    high = item.astype(jnp.bfloat16).astype(jnp.float32)
    return high, item - high


def grant(mib):
    return pltpu.CompilerParams(vmem_limit_bytes=mib * 1024 * 1024)


def turned(item):
    return (item.shape[1], item.shape[0]) + item.shape[2:]


def close(item):
    return pltpu.with_memory_space_constraint(item, pltpu.VMEM)


def pack_kernel(inner, spans, gate_ref, value_ref, write_ref, read_ref, *refs):
    outs, sems = refs[:inner], refs[inner]
    me = lax.rem(lax.axis_index("kv"), inner)
    copies = []
    for step in range(inner):
        target, low = me ^ step, 0
        for kind, ref in enumerate((gate_ref, value_ref, write_ref, read_ref)):
            span = spans[kind]
            first = pl.multiple_of(target * span, span)
            copies.append(
                pltpu.make_async_copy(
                    ref.at[:, pl.ds(first, span)],
                    outs[step].at[:, low : low + span],
                    sems.at[step * 4 + kind],
                )
            )
            low = low + span
    for copy in copies:
        copy.start()
    for copy in copies:
        copy.wait()


def make_packed(weights, spans, inner):
    depth = weights[0].shape[0]
    return pl.pallas_call(
        functools.partial(pack_kernel, inner, spans),
        in_specs=[pl.BlockSpec(memory_space=pltpu.HBM)] * 4,
        out_specs=[pl.BlockSpec(memory_space=pltpu.VMEM)] * inner,
        out_shape=[pltpu.VMEM((depth, sum(spans)), jnp.bfloat16)] * inner,
        scratch_shapes=[pltpu.SemaphoreType.DMA((4 * inner,))],
        compiler_params=grant(4),
        name="pack",
    )(*[pltpu.with_memory_space_constraint(item, pltpu.HBM) for item in weights])


def partial_kernel(inner, rows_ref, *refs):
    weights, out_ref = refs[:inner], refs[inner]
    depth = weights[0].shape[0]
    me = lax.rem(lax.axis_index("kv"), inner)
    total = None
    for step in range(inner):
        first = pl.multiple_of((me ^ step) * depth, depth)
        term = jnp.dot(
            rows_ref[:, pl.ds(first, depth)],
            weights[step][...],
            preferred_element_type=jnp.float32,
        )
        total = term if total is None else total + term
    out_ref[...] = total.astype(jnp.bfloat16)


def make_partial(rows, weights):
    count, width = rows.shape[0], weights[0].shape[1]
    vmem = pl.BlockSpec(memory_space=pltpu.VMEM)
    return pl.pallas_call(
        functools.partial(partial_kernel, len(weights)),
        in_specs=[vmem] * (1 + len(weights)),
        out_specs=vmem,
        out_shape=pltpu.VMEM((count, width), jnp.bfloat16),
        cost_estimate=pl.CostEstimate(
            flops=2 * rows.size * width, bytes_accessed=2 * count * width, transcendentals=0
        ),
        compiler_params=grant(12),
        name="partial",
    )(close(rows), *[close(item) for item in weights])


def root_kernel(
    taken_ref,
    base_ref,
    past_x_ref,
    past_b_ref,
    past_dt_ref,
    conv_x_ref,
    conv_b_ref,
    bias_ref,
    decay_ref,
    root_ref,
    short_ref,
):
    _, heads, width, states = base_ref.shape
    steps = past_dt_ref.shape[1]
    groups = past_b_ref.shape[2] // states
    span = heads * width // groups
    taken = taken_ref[pl.program_id(0)]
    copies = spread(heads, width)
    fixed = jnp.dot(
        jnp.concatenate([bias_ref[...], decay_ref[...]], axis=0),
        copies,
        precision=lax.Precision.HIGHEST,
        preferred_element_type=jnp.float32,
    )
    step = jnp.dot(
        past_dt_ref[0], copies.astype(jnp.bfloat16), preferred_element_type=jnp.float32
    )
    dt = softplus(step + fixed[0:1])
    live = lax.broadcasted_iota(jnp.int32, dt.shape, 0) < taken
    logs = jnp.where(live, -jnp.exp(fixed[1:2]) * dt, 0.0)
    tails = [jnp.zeros_like(logs[0:1])]
    for row in range(steps - 1, 0, -1):
        tails.insert(0, tails[0] + logs[row : row + 1])
    total = tails[0] + logs[0:1]
    weight = jnp.where(live, jnp.exp(jnp.concatenate(tails, axis=0)) * dt, 0.0)

    def conv(rows, taps):
        return sum(taps[k : k + 1] * rows[k : k + steps] for k in range(CONV_W))

    left = weight * silu(conv(past_x_ref[0].astype(jnp.float32), conv_x_ref[...]))
    right = silu(conv(past_b_ref[0].astype(jnp.float32), conv_b_ref[...]))
    left_high, left_low = halves_of(left)
    right_high, right_low = halves_of(right)
    scale = jnp.exp(total)
    scale_high, rest = halves_of(scale)
    scale_mid, rest = halves_of(rest)
    lhs = jnp.concatenate(
        [left_high, left_high, left_low, scale_high, scale_mid, rest, jnp.zeros_like(rest)], axis=0
    ).astype(jnp.bfloat16)
    rhs = jnp.concatenate([right_high, right_low, right_high], axis=0)
    rhs = jnp.concatenate([rhs, jnp.zeros((4, rhs.shape[1]), jnp.float32)], axis=0).astype(
        jnp.bfloat16
    )
    row = lax.broadcasted_iota(jnp.int32, (3 * steps + 4, states), 0)
    ones = jnp.where((row >= 3 * steps) & (row < 3 * steps + 3), 1.0, 0.0).astype(jnp.bfloat16)
    each = heads // groups
    for group in range(groups):
        both = lax.dot_general(
            lhs[:, group * span : (group + 1) * span],
            jnp.concatenate([rhs[:, group * states : (group + 1) * states], ones], axis=1),
            (((0,), (0,)), ((), ())),
            preferred_element_type=jnp.float32,
        )
        base = base_ref[0, group * each : (group + 1) * each].reshape(span, states)
        root = both[:, states:] * base + both[:, :states]
        root_ref[0, group * each : (group + 1) * each] = root.reshape(each, width, states)
        short_ref[0, group * span : (group + 1) * span] = root.astype(jnp.bfloat16)


def make_root(base, past_x, past_b, past_dt, taken, conv_x, conv_b, bias, decay):
    count, heads, width, states = base.shape

    def one(*dims):
        return pl.BlockSpec((1,) + dims, lambda s: (s,) + (0,) * len(dims))

    def same(item):
        return pl.BlockSpec(item.shape, lambda s: (0,) * item.ndim)

    args = (past_x, past_b, past_dt)
    fixed = (conv_x, conv_b, bias[None], decay[None])
    return pl.pallas_call(
        root_kernel,
        grid=(count,),
        in_specs=[pl.BlockSpec(memory_space=pltpu.SMEM), one(*base.shape[1:])]
        + [one(*item.shape[1:]) for item in args]
        + [same(item) for item in fixed],
        out_specs=[one(*base.shape[1:]), one(heads * width, states)],
        out_shape=[
            jax.ShapeDtypeStruct(base.shape, jnp.float32),
            jax.ShapeDtypeStruct((count, heads * width, states), jnp.bfloat16),
        ],
        cost_estimate=pl.CostEstimate(
            flops=4 * base.size * 16, bytes_accessed=10 * base.size, transcendentals=0
        ),
        compiler_params=grant(16),
        name="root",
    )(taken, base, *args, *fixed)


def mixer_kernel(
    outer,
    inner,
    spans,
    taken_ref,
    parts_ref,
    short_ref,
    step_ref,
    past_x_ref,
    past_b_ref,
    past_c_ref,
    conv_x_ref,
    conv_b_ref,
    conv_c_ref,
    bias_ref,
    decay_ref,
    skip_ref,
    gain_ref,
    out_ref,
    next_x_ref,
    next_b_ref,
    next_c_ref,
    now_ref,
    rows_x_ref,
    rows_b_ref,
    rows_c_ref,
    sems,
):
    count, kept, channels = past_x_ref.shape
    tokens = step_ref.shape[0]
    steps = tokens // count
    heads = bias_ref.shape[1]
    states = short_ref.shape[2]
    groups = past_b_ref.shape[2] // states
    span = channels // groups
    starts = (0, channels, 2 * channels, 2 * channels + groups * states)

    for block in range(inner):
        for kind in range(4):
            low = sum(spans[:kind])
            total = None
            for shard in range(outer):
                term = parts_ref[shard * inner + block, :, low : low + spans[kind]].astype(
                    jnp.float32
                )
                total = term if total is None else total + term
            first = starts[kind] + block * spans[kind]
            now_ref[:, first : first + spans[kind]] = total.astype(jnp.bfloat16)

    stride = kept + 1

    def pick(rows, source_of, columns):
        row = lax.broadcasted_iota(jnp.int32, (rows, columns), 0)
        column = lax.broadcasted_iota(jnp.int32, (rows, columns), 1)
        return source_of(row, column)

    def from_past(row, column):
        found = jnp.zeros(row.shape, jnp.bool_)
        for s in range(count):
            place, seq = window_place(row)
            hit = (seq == s) & (place < CONV_W - 1)
            found = found | (hit & (column == s * stride + taken_ref[s] + place))
        return jnp.where(found, 1.0, 0.0).astype(jnp.bfloat16)

    def from_now(row, column):
        place, seq = window_place(row)
        hit = (place >= CONV_W - 1) & (place < kept)
        hit = hit & (column == seq * steps + place - (CONV_W - 1))
        return jnp.where(hit, 1.0, 0.0).astype(jnp.bfloat16)

    def window_place(row):
        tap, token = row // tokens, row % tokens
        other = row - CONV_W * tokens
        is_tap = row < CONV_W * tokens
        place = jnp.where(is_tap, tap + token % steps, other // count)
        seq = jnp.where(is_tap, token // steps, other % count)
        return place, seq

    rows = CONV_W * tokens + count * kept
    pick_past = pick(rows, from_past, count * stride)
    pick_now = pick(rows, from_now, tokens)

    moves = []

    def window(past_ref, first, taps_ref, next_ref, rows_ref):
        size = past_ref.shape[2]
        past = jnp.concatenate(
            [
                jnp.concatenate(
                    [past_ref[s].astype(jnp.float32), jnp.zeros((1, size), jnp.float32)], axis=0
                )
                for s in range(count)
            ],
            axis=0,
        ).astype(jnp.bfloat16)
        picked = jnp.dot(pick_past, past, preferred_element_type=jnp.float32) + jnp.dot(
            pick_now, now_ref[:, first : first + size], preferred_element_type=jnp.float32
        )
        for row in range(kept):
            low = CONV_W * tokens + row * count
            rows_ref[row] = picked[low : low + count].astype(jnp.bfloat16)
        moves.append(pltpu.make_async_copy(rows_ref, next_ref, sems.at[len(moves)]))
        moves[-1].start()
        return silu(
            sum(
                taps_ref[k : k + 1] * picked[k * tokens : (k + 1) * tokens] for k in range(CONV_W)
            )
        )

    x = window(past_x_ref, starts[1], conv_x_ref, next_x_ref, rows_x_ref)
    b = window(past_b_ref, starts[2], conv_b_ref, next_b_ref, rows_b_ref)
    c = window(past_c_ref, starts[3], conv_c_ref, next_c_ref, rows_c_ref)

    copies = spread(heads, channels // heads)
    fixed = jnp.dot(
        jnp.concatenate([bias_ref[...], decay_ref[...], skip_ref[...]], axis=0),
        copies,
        precision=lax.Precision.HIGHEST,
        preferred_element_type=jnp.float32,
    )
    dt = softplus(
        jnp.dot(step_ref[...], copies.astype(jnp.bfloat16), preferred_element_type=jnp.float32)
        + fixed[0:1]
    )
    one = -jnp.exp(fixed[1:2]) * dt
    place = lax.broadcasted_iota(jnp.int32, (tokens, 1), 0) % steps
    seq = lax.broadcasted_iota(jnp.int32, (tokens, 1), 0) // steps
    logs = one
    for back in range(1, steps):
        logs = logs + jnp.where(place >= back, pltpu.roll(one, back, 0), 0.0)

    c_short = c.astype(jnp.bfloat16)
    carried = []
    for group in range(groups):
        total = None
        for s in range(count):
            term = lax.dot_general(
                c_short[:, group * states : (group + 1) * states],
                short_ref[s, group * span : (group + 1) * span],
                (((1,), (1,)), ((), ())),
                preferred_element_type=jnp.float32,
            )
            total = term if total is None else jnp.where(seq == s, term, total)
        carried.append(total)
    y = jnp.exp(logs) * jnp.concatenate(carried, axis=1) + fixed[2:3] * x
    for back in range(steps):
        other_b = pltpu.roll(b, back, 0) if back else b
        score = jnp.concatenate(
            [
                jnp.broadcast_to(
                    jnp.sum(
                        (c * other_b)[:, g * states : (g + 1) * states], axis=1, keepdims=True
                    ),
                    (tokens, span),
                )
                for g in range(groups)
            ],
            axis=1,
        )
        if back:
            drop = jnp.where(place >= back, logs - pltpu.roll(logs, back, 0), 0.0)
            term = jnp.exp(drop) * score * pltpu.roll(dt * x, back, 0)
            y = y + jnp.where(place >= back, term, 0.0)
        else:
            y = y + score * (dt * x)
    g = y * silu(now_ref[:, 0:channels].astype(jnp.float32))
    for group in range(groups):
        cols = slice(group * span, (group + 1) * span)
        part = g[:, cols]
        mean = jnp.sum(part * part, axis=1, keepdims=True) * (1.0 / span)
        out_ref[:, cols] = (part * lax.rsqrt(mean + EPSILON) * gain_ref[:, cols]).astype(
            jnp.bfloat16
        )
    for move in moves:
        move.wait()


def make_mixer(outer, inner, spans, taken, parts, short, step, pasts, convs, vectors):
    tokens = step.shape[0]
    args = (close(parts), short, step) + pasts + convs + tuple(item[None] for item in vectors)
    channels = pasts[0].shape[2]
    vmem = pl.BlockSpec(memory_space=pltpu.VMEM)
    return pl.pallas_call(
        functools.partial(mixer_kernel, outer, inner, spans),
        in_specs=[pl.BlockSpec(memory_space=pltpu.SMEM)] + [vmem] * len(args),
        out_specs=[vmem] + [pl.BlockSpec(memory_space=pltpu.HBM)] * 3,
        out_shape=[pltpu.VMEM((tokens, channels), jnp.bfloat16)]
        + [jax.ShapeDtypeStruct(turned(item), jnp.bfloat16) for item in pasts],
        scratch_shapes=[
            pltpu.VMEM((tokens, sum(item.shape[2] for item in pasts) + channels), jnp.bfloat16)
        ]
        + [pltpu.VMEM(turned(item), jnp.bfloat16) for item in pasts]
        + [pltpu.SemaphoreType.DMA((3,))],
        cost_estimate=pl.CostEstimate(
            flops=4 * short.size * tokens, bytes_accessed=2 * short.size, transcendentals=0
        ),
        compiler_params=grant(12),
        name="mixer",
    )(taken, *args)


def product_kernel(outer, inner, *refs):
    ys, columns, out_ref = refs[:outer], refs[outer : outer + inner], refs[outer + inner]
    stacked = jnp.concatenate([item[...] for item in ys], axis=0)
    size = columns[0].shape[1]
    for step in range(inner):
        result = jnp.dot(stacked, columns[step][...], preferred_element_type=jnp.float32)
        out_ref[:, step * size : (step + 1) * size] = result.astype(jnp.bfloat16)


def make_product(ys, columns):
    outer, inner = len(ys), len(columns)
    tokens, depth = ys[0].shape
    size = columns[0].shape[1]
    vmem = pl.BlockSpec(memory_space=pltpu.VMEM)
    return pl.pallas_call(
        functools.partial(product_kernel, outer, inner),
        in_specs=[vmem] * (outer + inner),
        out_specs=vmem,
        out_shape=pltpu.VMEM((outer * tokens, inner * size), jnp.bfloat16),
        cost_estimate=pl.CostEstimate(
            flops=2 * outer * tokens * depth * inner * size,
            bytes_accessed=2 * depth * inner * size,
            transcendentals=0,
        ),
        compiler_params=grant(6),
        name="product",
    )(*[close(item) for item in (*ys, *columns)])


def join_kernel(left_ref, right_ref, *outs):
    tokens = outs[0].shape[0]
    for shard, out in enumerate(outs):
        rows = slice(shard * tokens, (shard + 1) * tokens)
        total = left_ref[rows].astype(jnp.float32) + right_ref[rows].astype(jnp.float32)
        out[...] = total.astype(jnp.bfloat16)


def make_joined(left, right, outer):
    tokens, columns = left.shape
    vmem = pl.BlockSpec(memory_space=pltpu.VMEM)
    return pl.pallas_call(
        join_kernel,
        in_specs=[vmem] * 2,
        out_specs=[vmem] * outer,
        out_shape=[pltpu.VMEM((tokens // outer, columns), jnp.bfloat16)] * outer,
        compiler_params=grant(2),
        name="join",
    )(close(left), close(right))


def arrange_kernel(outer, inner, *refs):
    out_ref = refs[outer]
    count, steps, _ = out_ref.shape
    size = refs[0].shape[1] // inner
    half = outer // 2
    me, side = lax.axis_index("kv"), lax.axis_index("tp")
    me_outer, me_inner = lax.div(me, inner), lax.rem(me, inner)
    for step in range(outer):
        shard = me_outer ^ step

        @pl.when(lax.div(shard, half) == side)
        def _(step=step, shard=shard):
            item = refs[step][...].astype(jnp.float32)
            for sub in range(inner):
                column = (lax.rem(shard, half) * inner + (me_inner ^ sub)) * size
                column = pl.multiple_of(column, size)
                for s in range(count):
                    block = item[s * steps : (s + 1) * steps, sub * size : (sub + 1) * size]
                    out_ref[s, :, pl.ds(column, size)] = block.astype(jnp.bfloat16)


def make_arranged(items, inner, count):
    outer = len(items)
    tokens, columns = items[0].shape
    vmem = pl.BlockSpec(memory_space=pltpu.VMEM)
    return pl.pallas_call(
        functools.partial(arrange_kernel, outer, inner),
        in_specs=[vmem] * outer,
        out_specs=vmem,
        out_shape=jax.ShapeDtypeStruct(
            (count, tokens // count, outer // 2 * columns), jnp.bfloat16
        ),
        compiler_params=grant(2),
        name="arrange",
    )(*[close(item) for item in items])


def inner_size(ranks):
    size = 1
    while ranks % (2 * size) == 0 and 4 * size * size <= ranks:
        size = 2 * size
    return size


def swap(item, step):
    ranks = lax.axis_size("kv")
    return lax.ppermute(item, "kv", [(k, k ^ step) for k in range(ranks)])


def whole_step(
    tokens,
    input_gain,
    gate_weight,
    value_weight,
    write_weight,
    read_weight,
    step_weight,
    conv_value,
    conv_write,
    conv_read,
    step_bias,
    decay_log,
    skip_gain,
    output_gain,
    out_weight,
    base_state,
    past_value,
    past_write,
    past_read,
    past_step,
    accepted,
):
    ranks = lax.axis_size("kv")
    halves = lax.axis_size("tp")
    me = lax.axis_index("kv")
    side = lax.axis_index("tp")
    inner = inner_size(ranks)
    outer = ranks // inner
    me_inner = lax.rem(me, inner)
    me_outer = lax.div(me, inner)

    weights = (gate_weight, value_weight, write_weight, read_weight)
    spans = [item.shape[1] // inner for item in weights]

    def piece(step):
        target = me_inner ^ step
        return jnp.concatenate(
            [
                lax.dynamic_slice_in_dim(item, target * span, span, 1)
                for item, span in zip(weights, spans)
            ],
            axis=1,
        )

    if any(span % 128 for span in spans):
        packed = [piece(step) for step in range(inner)]
    else:
        packed = make_packed(weights, tuple(spans), inner)
    narrow = [packed[0]]
    for step in range(1, inner):
        narrow.append(swap(packed[step], step))

    whole = lax.all_gather(tokens, "tp", axis=2, tiled=True)
    seq_local, proposals, width = whole.shape
    rows = whole.astype(jnp.float32)
    normed = (
        rows * lax.rsqrt(jnp.mean(rows * rows, axis=-1, keepdims=True) + EPSILON) * input_gain
    ).astype(jnp.bfloat16)
    flat = normed.reshape(seq_local * proposals, width)
    token_count = flat.shape[0]
    head_count = step_bias.shape[0]
    own_step = lax.dynamic_slice_in_dim(step_weight, side * head_count, head_count, 1)
    step_now = jnp.dot(flat, own_step, preferred_element_type=jnp.float32).astype(jnp.bfloat16)

    part = width // (outer * halves)
    share = lax.dynamic_index_in_dim(
        flat.reshape(token_count, outer, halves, part), side, 2, keepdims=False
    )
    share = jnp.broadcast_to(
        jnp.swapaxes(share, 0, 1)[:, None], (outer, inner, token_count, part)
    ).reshape(ranks * token_count, part)
    everyone = lax.all_to_all(share, "kv", split_axis=0, concat_axis=0, tiled=True)
    everyone = lax.all_gather(everyone, "tp", axis=1, tiled=True)

    block = width // ranks
    if block % 128 or sum(spans) % 128:
        product = None
        for step in range(inner):
            term = jnp.dot(
                lax.dynamic_slice_in_dim(everyone, (me_inner ^ step) * block, block, 1),
                narrow[step],
                preferred_element_type=jnp.float32,
            )
            product = term if product is None else product + term
        product = product.astype(jnp.bfloat16)
    else:
        product = make_partial(everyone, narrow)
    returned = lax.all_to_all(product, "kv", split_axis=0, concat_axis=0, tiled=True)
    columns = [out_weight]
    for step in range(1, inner):
        columns.append(swap(out_weight, step))
    returned = returned.reshape(ranks, token_count, sum(spans))
    shards, pieces = outer, inner
    if any(span % 128 for span in spans):
        summed = jnp.sum(
            returned.reshape(outer, inner, token_count, sum(spans)).astype(jnp.float32), axis=0
        ).astype(jnp.bfloat16)
        joined, offset = [], 0
        for span in spans:
            item = jnp.swapaxes(summed[:, :, offset : offset + span], 0, 1)
            joined.append(item.reshape(token_count, inner * span))
            offset = offset + span
        returned = jnp.concatenate(joined, axis=1)[None]
        spans = [inner * span for span in spans]
        shards, pieces = 1, 1

    root_state, short = make_root(
        base_state,
        past_value,
        past_write,
        past_step,
        accepted,
        conv_value,
        conv_write,
        step_bias,
        decay_log,
    )
    flat_y, *nexts = make_mixer(
        shards,
        pieces,
        tuple(spans),
        accepted,
        returned,
        short,
        step_now,
        (past_value, past_write, past_read),
        (conv_value, conv_write, conv_read),
        (step_bias, decay_log, skip_gain, output_gain),
    )
    next_value, next_write, next_read = [jnp.swapaxes(item, 0, 1) for item in nexts]
    ys = [flat_y] + [swap(flat_y, inner * step) for step in range(1, outer)]
    step_out = step_now.reshape(seq_local, proposals, head_count)
    if out_weight.shape[1] % 128 == 0 and halves == 2 and outer % 2 == 0:
        partial = make_product(ys, columns)
        keeper = [(k // inner) // (outer // 2) for k in range(ranks)]
        other = lax.ppermute(
            partial, ("kv", "tp"), [(2 * k + 1 - keeper[k], 2 * k + keeper[k]) for k in range(ranks)]
        )
        sums = make_joined(partial, other, outer)
        blocks = [sums[0]] + [
            lax.ppermute(
                sums[step],
                ("kv", "tp"),
                [(2 * k + keeper[k], 2 * (k ^ (inner * step)) + keeper[k]) for k in range(ranks)],
            )
            for step in range(1, outer)
        ]
        mixed = make_arranged(blocks, inner, seq_local)
        return (mixed, root_state, next_value, next_write, next_read, step_out)
    stacked = jnp.concatenate(ys, axis=0)
    partial = jnp.concatenate(
        [
            jnp.dot(stacked, item, preferred_element_type=jnp.float32).astype(jnp.bfloat16)
            for item in columns
        ],
        axis=1,
    ).reshape(outer, token_count, -1)
    blocks = jnp.stack(
        [partial[0]] + [swap(partial[step], inner * step) for step in range(1, outer)]
    ).reshape(outer, token_count, inner, -1)
    order_outer = me_outer ^ jnp.arange(outer)
    order_inner = me_inner ^ jnp.arange(inner)
    blocks = jnp.take(jnp.take(blocks, order_outer, axis=0), order_inner, axis=2)
    full = jnp.swapaxes(blocks, 0, 1).reshape(token_count, halves, width // halves)
    shares = lax.all_to_all(full, "tp", split_axis=1, concat_axis=1, tiled=True)
    mixed = jnp.sum(shares.astype(jnp.float32), axis=1).astype(jnp.bfloat16)
    mixed = mixed.reshape(seq_local, proposals, width // halves)
    return (mixed, root_state, next_value, next_write, next_read, step_out)


def solution(mesh):
    return jax.shard_map(
        whole_step,
        mesh=mesh,
        in_specs=(
            P("kv", None, "tp"),
            P(),
            P("kv", "tp"),
            P("kv", "tp"),
            P("kv", "tp"),
            P("kv", "tp"),
            P(),
            P(None, "tp"),
            P(None, "tp"),
            P(None, "tp"),
            P("tp"),
            P("tp"),
            P("tp"),
            P("tp"),
            P("tp", "kv"),
            P("kv", "tp", None, None),
            P("kv", None, "tp"),
            P("kv", None, "tp"),
            P("kv", None, "tp"),
            P("kv", None, "tp"),
            P("kv"),
        ),
        out_specs=(
            P("kv", None, "tp"),
            P("kv", "tp", None, None),
            P("kv", None, "tp"),
            P("kv", None, "tp"),
            P("kv", None, "tp"),
            P("kv", None, "tp"),
        ),
        check_vma=False,
    )
```

```python
import functools

import jax
import jax.numpy as jnp
from jax import lax
from jax.experimental import pallas as pl
from jax.experimental.pallas import tpu as pltpu
from jax.sharding import PartitionSpec as P


CONV_W = 4
EPSILON = 1e-06


def silu(v):
    return v / (1.0 + jnp.exp(-v))


def softplus(v):
    return jnp.maximum(v, 0.0) + jnp.log1p(jnp.exp(-jnp.abs(v)))


def spread(heads, width):
    lane = lax.broadcasted_iota(jnp.int32, (heads, heads * width), 1)
    head = lax.broadcasted_iota(jnp.int32, (heads, heads * width), 0)
    return jnp.where(lane // width == head, 1.0, 0.0)


def halves_of(item):
    high = item.astype(jnp.bfloat16).astype(jnp.float32)
    return high, item - high


def grant(mib):
    return pltpu.CompilerParams(vmem_limit_bytes=mib * 1024 * 1024)


def apart(item):
    return pltpu.with_memory_space_constraint(item, pltpu.HBM)


def close(item):
    return pltpu.with_memory_space_constraint(item, pltpu.VMEM)


def pack_kernel(inner, spans, gate_ref, value_ref, write_ref, read_ref, *refs):
    outs, sems = refs[:inner], refs[inner]
    me = lax.rem(lax.axis_index("kv"), inner)
    copies = []
    for step in range(inner):
        target, low = me ^ step, 0
        for kind, ref in enumerate((gate_ref, value_ref, write_ref, read_ref)):
            span = spans[kind]
            first = pl.multiple_of(target * span, span)
            copies.append(
                pltpu.make_async_copy(
                    ref.at[:, pl.ds(first, span)],
                    outs[step].at[:, low : low + span],
                    sems.at[step * 4 + kind],
                )
            )
            low = low + span
    for copy in copies:
        copy.start()
    for copy in copies:
        copy.wait()


def make_packed(weights, spans, inner):
    depth = weights[0].shape[0]
    return pl.pallas_call(
        functools.partial(pack_kernel, inner, spans),
        in_specs=[pl.BlockSpec(memory_space=pltpu.HBM)] * 4,
        out_specs=[pl.BlockSpec(memory_space=pltpu.VMEM)] * inner,
        out_shape=[pltpu.VMEM((depth, sum(spans)), jnp.bfloat16)] * inner,
        scratch_shapes=[pltpu.SemaphoreType.DMA((4 * inner,))],
        compiler_params=grant(4),
        name="pack",
    )(*[pltpu.with_memory_space_constraint(item, pltpu.HBM) for item in weights])


def partial_kernel(inner, rows_ref, *refs):
    weights, out_ref = refs[:inner], refs[inner]
    depth = weights[0].shape[0]
    me = lax.rem(lax.axis_index("kv"), inner)
    total = None
    for step in range(inner):
        first = pl.multiple_of((me ^ step) * depth, depth)
        term = jnp.dot(
            rows_ref[:, pl.ds(first, depth)],
            weights[step][...],
            preferred_element_type=jnp.float32,
        )
        total = term if total is None else total + term
    out_ref[...] = total.astype(jnp.bfloat16)


def make_partial(rows, weights):
    count, width = rows.shape[0], weights[0].shape[1]
    vmem = pl.BlockSpec(memory_space=pltpu.VMEM)
    return pl.pallas_call(
        functools.partial(partial_kernel, len(weights)),
        in_specs=[vmem] * (1 + len(weights)),
        out_specs=vmem,
        out_shape=pltpu.VMEM((count, width), jnp.bfloat16),
        cost_estimate=pl.CostEstimate(
            flops=2 * rows.size * width, bytes_accessed=2 * count * width, transcendentals=0
        ),
        compiler_params=grant(12),
        name="partial",
    )(close(rows), *[close(item) for item in weights])


def hold_kernel(from_ref, to_ref, sem):
    copy = pltpu.make_async_copy(from_ref, to_ref, sem)
    copy.start()
    copy.wait()


def make_held(item):
    return pl.pallas_call(
        hold_kernel,
        in_specs=[pl.BlockSpec(memory_space=pltpu.HBM)],
        out_specs=pl.BlockSpec(memory_space=pltpu.VMEM),
        out_shape=pltpu.VMEM(item.shape, item.dtype),
        scratch_shapes=[pltpu.SemaphoreType.DMA],
        cost_estimate=pl.CostEstimate(
            flops=item.size * 64, bytes_accessed=4 * item.size, transcendentals=0
        ),
        compiler_params=grant(2),
        name="hold",
    )(apart(item))


def place_in(rows, cols, source):
    row = lax.broadcasted_iota(jnp.int32, (rows, cols), 0)
    column = lax.broadcasted_iota(jnp.int32, (rows, cols), 1)
    return jnp.where(column == source(row), 1.0, 0.0).astype(jnp.bfloat16)


def stacked_rows(ref):
    rows = [ref[k].astype(jnp.float32) for k in range(ref.shape[0])]
    return jnp.concatenate(rows, axis=0).astype(jnp.bfloat16)


def root_kernel(
    taken_ref,
    base_ref,
    past_x_ref,
    past_b_ref,
    past_dt_ref,
    conv_x_ref,
    conv_b_ref,
    bias_ref,
    decay_ref,
    rows_ref,
    step_weight_ref,
    root_ref,
    short_ref,
    step_ref,
    step_out_ref,
    lhs_ref,
    rhs_ref,
):
    _, heads, width, states = base_ref.shape
    count, steps = past_dt_ref.shape[:2]
    tokens = count * steps
    groups = past_b_ref.shape[2] // states
    span = heads * width // groups
    each = heads // groups

    @pl.when(pl.program_id(0) == 0)
    def _():
        first = 0
        if step_weight_ref.shape[0] > heads:
            first = pl.multiple_of(lax.axis_index("tp") * heads, heads)
        step = lax.dot_general(
            stacked_rows(rows_ref),
            step_weight_ref[pl.ds(first, heads), :],
            (((1,), (1,)), ((), ())),
            preferred_element_type=jnp.float32,
        )
        step_ref[...] = step.astype(jnp.bfloat16)
        for s in range(count):
            step_out_ref[s] = step[s * steps : (s + 1) * steps].astype(jnp.bfloat16)

        copies = spread(heads, width)
        fixed = jnp.dot(
            jnp.concatenate([bias_ref[...], decay_ref[...]], axis=0),
            copies,
            precision=lax.Precision.HIGHEST,
            preferred_element_type=jnp.float32,
        )
        past_dt = jnp.dot(
            stacked_rows(past_dt_ref),
            copies.astype(jnp.bfloat16),
            preferred_element_type=jnp.float32,
        )
        dt = softplus(past_dt + fixed[0:1])
        row = lax.broadcasted_iota(jnp.int32, (tokens, 1), 0)
        place = row % steps
        taken = jnp.zeros_like(row)
        for s in range(count):
            taken = jnp.where(row // steps == s, taken_ref[s], taken)
        live = place < taken
        logs = jnp.where(live, -jnp.exp(fixed[1:2]) * dt, 0.0)
        tail = jnp.zeros_like(logs)
        for ahead in range(1, steps):
            moved = pltpu.roll(logs, tokens - ahead, 0)
            tail = tail + jnp.where(place + ahead < steps, moved, 0.0)
        weight = jnp.where(live, jnp.exp(tail) * dt, 0.0)
        scale = jnp.exp(tail + logs)

        pick = place_in(
            CONV_W * tokens,
            past_x_ref.shape[0] * count,
            lambda r: (r // tokens + r % steps) * count + (r % tokens) // steps,
        )

        def conv(past_ref, taps_ref):
            rows = jnp.dot(pick, stacked_rows(past_ref), preferred_element_type=jnp.float32)
            return silu(
                sum(
                    taps_ref[k : k + 1] * rows[k * tokens : (k + 1) * tokens]
                    for k in range(CONV_W)
                )
            )

        left_high, left_low = halves_of(weight * conv(past_x_ref, conv_x_ref))
        right_high, right_low = halves_of(conv(past_b_ref, conv_b_ref))
        scale_high, rest = halves_of(scale)
        scale_mid, rest = halves_of(rest)
        for s in range(count):
            all_rows = slice(s * steps, (s + 1) * steps)
            one = slice(s * steps, s * steps + 1)
            lhs_ref[s] = jnp.concatenate(
                [left_high[all_rows], left_high[all_rows], left_low[all_rows]]
                + [scale_high[one], scale_mid[one], rest[one], jnp.zeros_like(rest[one])],
                axis=0,
            ).astype(jnp.bfloat16)
            rhs_ref[s] = jnp.concatenate(
                [right_high[all_rows], right_low[all_rows], right_high[all_rows]]
                + [jnp.zeros((4, rhs_ref.shape[2]), jnp.float32)],
                axis=0,
            ).astype(jnp.bfloat16)

    lhs, rhs = lhs_ref[pl.program_id(0)], rhs_ref[pl.program_id(0)]
    row = lax.broadcasted_iota(jnp.int32, (3 * steps + 4, states), 0)
    ones = jnp.where((row >= 3 * steps) & (row < 3 * steps + 3), 1.0, 0.0).astype(jnp.bfloat16)
    for group in range(groups):
        both = lax.dot_general(
            lhs[:, group * span : (group + 1) * span],
            jnp.concatenate([rhs[:, group * states : (group + 1) * states], ones], axis=1),
            (((0,), (0,)), ((), ())),
            preferred_element_type=jnp.float32,
        )
        base = base_ref[0, group * each : (group + 1) * each].reshape(span, states)
        root = both[:, states:] * base + both[:, :states]
        root_ref[0, group * each : (group + 1) * each] = root.reshape(each, width, states)
        rows = slice(group * span, (group + 1) * span)
        short_ref[pl.program_id(0), rows] = root.astype(jnp.bfloat16)


def make_root(base, past_x, past_b, past_dt, taken, conv_x, conv_b, bias, decay, rows, step_weight):
    count, heads, width, states = base.shape
    steps = past_dt.shape[1]

    def one(*dims):
        return pl.BlockSpec((1,) + dims, lambda s: (s,) + (0,) * len(dims))

    def same(*dims):
        return pl.BlockSpec(dims, lambda s: (0,) * len(dims))

    fixed = (past_x, past_b, past_dt, conv_x, conv_b, bias[None], decay[None], rows, step_weight)
    depth = 3 * steps + 4
    return pl.pallas_call(
        root_kernel,
        grid=(count,),
        in_specs=[pl.BlockSpec(memory_space=pltpu.SMEM), one(*base.shape[1:])]
        + [same(*item.shape) for item in fixed],
        out_specs=[
            one(*base.shape[1:]),
            pl.BlockSpec(memory_space=pltpu.VMEM),
            same(count * steps, heads),
            same(count, steps, heads),
        ],
        out_shape=[
            jax.ShapeDtypeStruct(base.shape, jnp.float32),
            pltpu.VMEM((count, heads * width, states), jnp.bfloat16),
            jax.ShapeDtypeStruct((count * steps, heads), jnp.bfloat16),
            jax.ShapeDtypeStruct((count, steps, heads), jnp.bfloat16),
        ],
        scratch_shapes=[
            pltpu.VMEM((count, depth, heads * width), jnp.bfloat16),
            pltpu.VMEM((count, depth, past_b.shape[2]), jnp.bfloat16),
        ],
        cost_estimate=pl.CostEstimate(
            flops=4 * base.size * 16, bytes_accessed=10 * base.size, transcendentals=0
        ),
        compiler_params=grant(16),
        name="root",
    )(taken, *[apart(item) for item in (base, *fixed)])


def mixer_kernel(
    outer,
    inner,
    spans,
    taken_ref,
    parts_ref,
    short_ref,
    step_ref,
    past_x_ref,
    past_b_ref,
    past_c_ref,
    conv_x_ref,
    conv_b_ref,
    conv_c_ref,
    bias_ref,
    decay_ref,
    skip_ref,
    gain_ref,
    out_ref,
    next_x_ref,
    next_b_ref,
    next_c_ref,
    now_ref,
    rows_x_ref,
    rows_b_ref,
    rows_c_ref,
    sems,
):
    kept, count, channels = past_x_ref.shape
    tokens = step_ref.shape[0]
    steps = tokens // count
    heads = bias_ref.shape[1]
    states = short_ref.shape[2]
    groups = past_b_ref.shape[2] // states
    span = channels // groups
    starts = (0, channels, 2 * channels, 2 * channels + groups * states)

    for block in range(inner):
        for kind in range(4):
            low = sum(spans[:kind])
            total = None
            for shard in range(outer):
                term = parts_ref[shard * inner + block, :, low : low + spans[kind]].astype(
                    jnp.float32
                )
                total = term if total is None else total + term
            first = starts[kind] + block * spans[kind]
            now_ref[:, first : first + spans[kind]] = total.astype(jnp.bfloat16)

    def pick(rows, source_of, columns):
        row = lax.broadcasted_iota(jnp.int32, (rows, columns), 0)
        column = lax.broadcasted_iota(jnp.int32, (rows, columns), 1)
        return source_of(row, column)

    def from_past(row, column):
        found = jnp.zeros(row.shape, jnp.bool_)
        for s in range(count):
            place, seq = window_place(row)
            hit = (seq == s) & (place < CONV_W - 1)
            found = found | (hit & (column == (taken_ref[s] + place) * count + s))
        return jnp.where(found, 1.0, 0.0).astype(jnp.bfloat16)

    def from_now(row, column):
        place, seq = window_place(row)
        hit = (place >= CONV_W - 1) & (place < kept)
        hit = hit & (column == seq * steps + place - (CONV_W - 1))
        return jnp.where(hit, 1.0, 0.0).astype(jnp.bfloat16)

    def window_place(row):
        tap, token = row // tokens, row % tokens
        other = row - CONV_W * tokens
        is_tap = row < CONV_W * tokens
        place = jnp.where(is_tap, tap + token % steps, other // count)
        seq = jnp.where(is_tap, token // steps, other % count)
        return place, seq

    rows = CONV_W * tokens + count * kept
    pick_past = pick(rows, from_past, kept * count)
    pick_now = pick(rows, from_now, tokens)

    moves = []

    def window(past_ref, first, taps_ref, next_ref, rows_ref):
        size = past_ref.shape[2]
        past = stacked_rows(past_ref)
        picked = jnp.dot(pick_past, past, preferred_element_type=jnp.float32) + jnp.dot(
            pick_now, now_ref[:, first : first + size], preferred_element_type=jnp.float32
        )
        for row in range(kept):
            low = CONV_W * tokens + row * count
            rows_ref[row] = picked[low : low + count].astype(jnp.bfloat16)
        moves.append(pltpu.make_async_copy(rows_ref, next_ref, sems.at[len(moves)]))
        moves[-1].start()
        return silu(
            sum(
                taps_ref[k : k + 1] * picked[k * tokens : (k + 1) * tokens] for k in range(CONV_W)
            )
        )

    x = window(past_x_ref, starts[1], conv_x_ref, next_x_ref, rows_x_ref)
    b = window(past_b_ref, starts[2], conv_b_ref, next_b_ref, rows_b_ref)
    c = window(past_c_ref, starts[3], conv_c_ref, next_c_ref, rows_c_ref)

    copies = spread(heads, channels // heads)
    fixed = jnp.dot(
        jnp.concatenate([bias_ref[...], decay_ref[...], skip_ref[...]], axis=0),
        copies,
        precision=lax.Precision.HIGHEST,
        preferred_element_type=jnp.float32,
    )
    dt = softplus(
        jnp.dot(step_ref[...], copies.astype(jnp.bfloat16), preferred_element_type=jnp.float32)
        + fixed[0:1]
    )
    one = -jnp.exp(fixed[1:2]) * dt
    place = lax.broadcasted_iota(jnp.int32, (tokens, 1), 0) % steps
    seq = lax.broadcasted_iota(jnp.int32, (tokens, 1), 0) // steps
    logs = one
    for back in range(1, steps):
        logs = logs + jnp.where(place >= back, pltpu.roll(one, back, 0), 0.0)

    c_short = c.astype(jnp.bfloat16)
    carried = []
    for group in range(groups):
        total = None
        for s in range(count):
            term = lax.dot_general(
                c_short[:, group * states : (group + 1) * states],
                short_ref[s, group * span : (group + 1) * span],
                (((1,), (1,)), ((), ())),
                preferred_element_type=jnp.float32,
            )
            total = term if total is None else jnp.where(seq == s, term, total)
        carried.append(total)
    y = jnp.exp(logs) * jnp.concatenate(carried, axis=1) + fixed[2:3] * x
    for back in range(steps):
        other_b = pltpu.roll(b, back, 0) if back else b
        score = jnp.concatenate(
            [
                jnp.broadcast_to(
                    jnp.sum(
                        (c * other_b)[:, g * states : (g + 1) * states], axis=1, keepdims=True
                    ),
                    (tokens, span),
                )
                for g in range(groups)
            ],
            axis=1,
        )
        if back:
            drop = jnp.where(place >= back, logs - pltpu.roll(logs, back, 0), 0.0)
            term = jnp.exp(drop) * score * pltpu.roll(dt * x, back, 0)
            y = y + jnp.where(place >= back, term, 0.0)
        else:
            y = y + score * (dt * x)
    g = y * silu(now_ref[:, 0:channels].astype(jnp.float32))
    for group in range(groups):
        cols = slice(group * span, (group + 1) * span)
        part = g[:, cols]
        mean = jnp.sum(part * part, axis=1, keepdims=True) * (1.0 / span)
        out_ref[:, cols] = (part * lax.rsqrt(mean + EPSILON) * gain_ref[:, cols]).astype(
            jnp.bfloat16
        )
    for move in moves:
        move.wait()


def make_mixer(outer, inner, spans, taken, parts, short, step, pasts, convs, vectors):
    tokens = step.shape[0]
    small = (step, *pasts, *convs, *[item[None] for item in vectors])
    args = (close(parts), close(short), *[apart(item) for item in small])
    channels = pasts[0].shape[2]
    vmem = pl.BlockSpec(memory_space=pltpu.VMEM)
    return pl.pallas_call(
        functools.partial(mixer_kernel, outer, inner, spans),
        in_specs=[pl.BlockSpec(memory_space=pltpu.SMEM)] + [vmem] * len(args),
        out_specs=[vmem] + [pl.BlockSpec(memory_space=pltpu.HBM)] * 3,
        out_shape=[pltpu.VMEM((tokens, channels), jnp.bfloat16)]
        + [jax.ShapeDtypeStruct(item.shape, jnp.bfloat16) for item in pasts],
        scratch_shapes=[
            pltpu.VMEM((tokens, sum(item.shape[2] for item in pasts) + channels), jnp.bfloat16)
        ]
        + [pltpu.VMEM(item.shape, jnp.bfloat16) for item in pasts]
        + [pltpu.SemaphoreType.DMA((3,))],
        cost_estimate=pl.CostEstimate(
            flops=4 * short.size * tokens, bytes_accessed=2 * short.size, transcendentals=0
        ),
        compiler_params=grant(12),
        name="mixer",
    )(taken, *args)


def product_kernel(outer, chunks, *refs):
    ys, columns, out_ref = refs[:outer], refs[outer:-1], refs[-1]
    stacked = jnp.concatenate([item[...] for item in ys], axis=0)
    size, at = columns[0].shape[1], 0
    for step, count in enumerate(chunks):
        total, row = None, 0
        for ref in columns[at : at + count]:
            term = jnp.dot(
                stacked[:, row : row + ref.shape[0]],
                ref[...],
                preferred_element_type=jnp.float32,
            )
            total = term if total is None else total + term
            row = row + ref.shape[0]
        out_ref[:, step * size : (step + 1) * size] = total.astype(jnp.bfloat16)
        at = at + count


def make_product(ys, columns):
    outer, inner = len(ys), len(columns)
    tokens, depth = ys[0].shape
    size = columns[0][0].shape[1]
    vmem = pl.BlockSpec(memory_space=pltpu.VMEM)
    items = [*ys, *[chunk for item in columns for chunk in item]]
    return pl.pallas_call(
        functools.partial(product_kernel, outer, tuple(len(item) for item in columns)),
        in_specs=[vmem] * len(items),
        out_specs=vmem,
        out_shape=pltpu.VMEM((outer * tokens, inner * size), jnp.bfloat16),
        cost_estimate=pl.CostEstimate(
            flops=2 * outer * tokens * depth * inner * size,
            bytes_accessed=2 * depth * inner * size,
            transcendentals=0,
        ),
        compiler_params=grant(6),
        name="product",
    )(*[close(item) for item in items])


def join_kernel(left_ref, right_ref, *outs):
    tokens = outs[0].shape[0]
    for shard, out in enumerate(outs):
        rows = slice(shard * tokens, (shard + 1) * tokens)
        total = left_ref[rows].astype(jnp.float32) + right_ref[rows].astype(jnp.float32)
        out[...] = total.astype(jnp.bfloat16)


def make_joined(left, right, outer):
    tokens, columns = left.shape
    vmem = pl.BlockSpec(memory_space=pltpu.VMEM)
    return pl.pallas_call(
        join_kernel,
        in_specs=[vmem] * 2,
        out_specs=[vmem] * outer,
        out_shape=[pltpu.VMEM((tokens // outer, columns), jnp.bfloat16)] * outer,
        compiler_params=grant(2),
        name="join",
    )(close(left), close(right))


def arrange_kernel(outs, ins, ranks, *refs):
    out_ref = refs[len(outs)]
    count, steps, _ = out_ref.shape
    size = refs[0].shape[1] // len(ins)
    half = ranks // 2
    me, side = lax.axis_index("kv"), lax.axis_index("tp")
    for place, out in enumerate(outs):

        @pl.when(lax.div(me ^ out, half) == side)
        def _(place=place, out=out):
            item = refs[place][...].astype(jnp.float32)
            for sub, step in enumerate(ins):
                column = lax.rem(me ^ (out ^ step), half) * size
                column = pl.multiple_of(column, size)
                for s in range(count):
                    block = item[s * steps : (s + 1) * steps, sub * size : (sub + 1) * size]
                    out_ref[s, :, pl.ds(column, size)] = block.astype(jnp.bfloat16)


def make_arranged(items, outs, ins, ranks, count):
    tokens, columns = items[0].shape
    vmem = pl.BlockSpec(memory_space=pltpu.VMEM)
    return pl.pallas_call(
        functools.partial(arrange_kernel, outs, ins, ranks),
        in_specs=[vmem] * len(outs),
        out_specs=vmem,
        out_shape=jax.ShapeDtypeStruct(
            (count, tokens // count, len(outs) // 2 * columns), jnp.bfloat16
        ),
        compiler_params=grant(2),
        name="arrange",
    )(*[close(item) for item in items])


def sums_of(bits):
    found = [0]
    for bit in bits:
        found = found + [item | bit for item in found]
    return tuple(found)


def inner_size(ranks):
    size = 1
    while ranks % (2 * size) == 0 and 4 * size * size <= ranks:
        size = 2 * size
    return size


def swap(item, step):
    ranks = lax.axis_size("kv")
    return lax.ppermute(item, "kv", [(k, k ^ step) for k in range(ranks)])


def whole_step(
    tokens,
    input_gain,
    gate_weight,
    value_weight,
    write_weight,
    read_weight,
    step_weight,
    conv_value,
    conv_write,
    conv_read,
    step_bias,
    decay_log,
    skip_gain,
    output_gain,
    out_weight,
    base_state,
    past_value,
    past_write,
    past_read,
    past_step,
    accepted,
):
    ranks = lax.axis_size("kv")
    halves = lax.axis_size("tp")
    me = lax.axis_index("kv")
    side = lax.axis_index("tp")
    inner = inner_size(ranks)
    outer = ranks // inner
    me_inner = lax.rem(me, inner)

    weights = (gate_weight, value_weight, write_weight, read_weight)
    spans = [item.shape[1] // inner for item in weights]

    def piece(step):
        target = me_inner ^ step
        return jnp.concatenate(
            [
                lax.dynamic_slice_in_dim(item, target * span, span, 1)
                for item, span in zip(weights, spans)
            ],
            axis=1,
        )

    if any(span % 128 for span in spans):
        packed = [piece(step) for step in range(inner)]
    else:
        packed = make_packed(weights, tuple(spans), inner)
    narrow = [packed[0]]
    for step in range(1, inner):
        narrow.append(swap(packed[step], step))

    whole = lax.all_gather(tokens, "tp", axis=2, tiled=True)
    seq_local, proposals, width = whole.shape
    rows = whole.astype(jnp.float32)
    normed = (
        rows * lax.rsqrt(jnp.mean(rows * rows, axis=-1, keepdims=True) + EPSILON) * input_gain
    ).astype(jnp.bfloat16)
    flat = normed.reshape(seq_local * proposals, width)
    token_count = flat.shape[0]
    head_count = step_bias.shape[0]
    part = width // (outer * halves)
    share = lax.dynamic_index_in_dim(
        flat.reshape(token_count, outer, halves, part), side, 2, keepdims=False
    )
    share = jnp.broadcast_to(
        jnp.swapaxes(share, 0, 1)[:, None], (outer, inner, token_count, part)
    ).reshape(ranks * token_count, part)
    everyone = lax.all_to_all(share, "kv", split_axis=0, concat_axis=0, tiled=True)
    everyone = lax.all_gather(everyone, "tp", axis=1, tiled=True)

    block = width // ranks
    if block % 128 or sum(spans) % 128:
        product = None
        for step in range(inner):
            term = jnp.dot(
                lax.dynamic_slice_in_dim(everyone, (me_inner ^ step) * block, block, 1),
                narrow[step],
                preferred_element_type=jnp.float32,
            )
            product = term if product is None else product + term
        product = product.astype(jnp.bfloat16)
    else:
        product = make_partial(everyone, narrow)
    returned = lax.all_to_all(product, "kv", split_axis=0, concat_axis=0, tiled=True)
    bits = [1 << k for k in range(ranks.bit_length() - 1)]
    ins, outs = sums_of(bits[0::2]), sums_of(bits[1::2])
    columns = [[out_weight]]
    if len(ins) == 4:
        near_bit, far_bit = bits[0], bits[2]
        far = swap(out_weight, far_bit)
        beside = swap(out_weight, near_bit)
        cut = out_weight.shape[0] // 2
        first = swap(far[:cut], near_bit)
        second = swap(beside[cut:], far_bit)
        columns = [[make_held(out_weight)], [beside], [far], [first, second]]
    else:
        for step in ins[1:]:
            columns.append([swap(out_weight, step)])
    returned = returned.reshape(ranks, token_count, sum(spans))
    shards, pieces = outer, inner
    if any(span % 128 for span in spans):
        summed = jnp.sum(
            returned.reshape(outer, inner, token_count, sum(spans)).astype(jnp.float32), axis=0
        ).astype(jnp.bfloat16)
        joined, offset = [], 0
        for span in spans:
            item = jnp.swapaxes(summed[:, :, offset : offset + span], 0, 1)
            joined.append(item.reshape(token_count, inner * span))
            offset = offset + span
        returned = jnp.concatenate(joined, axis=1)[None]
        spans = [inner * span for span in spans]
        shards, pieces = 1, 1

    past_value, past_write, past_read = [
        jnp.swapaxes(item, 0, 1) for item in (past_value, past_write, past_read)
    ]
    turned = jnp.swapaxes(step_weight, 0, 1)
    if head_count % 16:
        turned = lax.dynamic_slice_in_dim(turned, side * head_count, head_count, 0)
    root_state, short, step_now, step_out = make_root(
        base_state,
        past_value,
        past_write,
        past_step,
        accepted,
        conv_value,
        conv_write,
        step_bias,
        decay_log,
        normed,
        turned,
    )
    flat_y, *nexts = make_mixer(
        shards,
        pieces,
        tuple(spans),
        accepted,
        returned,
        short,
        step_now,
        (past_value, past_write, past_read),
        (conv_value, conv_write, conv_read),
        (step_bias, decay_log, skip_gain, output_gain),
    )
    next_value, next_write, next_read = [jnp.swapaxes(item, 0, 1) for item in nexts]
    ys = [flat_y] + [swap(flat_y, step) for step in outs[1:]]
    if out_weight.shape[1] % 128 == 0 and halves == 2 and bits[-1] in outs:
        partial = make_product(ys, columns)
        keeper = [k // (ranks // 2) for k in range(ranks)]
        other = lax.ppermute(
            partial, ("kv", "tp"), [(2 * k + 1 - keeper[k], 2 * k + keeper[k]) for k in range(ranks)]
        )
        sums = make_joined(partial, other, len(outs))
        blocks = [sums[0]]
        for place, step in enumerate(outs[1:], 1):
            pairs = [(2 * k + keeper[k], 2 * (k ^ step) + keeper[k]) for k in range(ranks)]
            blocks.append(lax.ppermute(sums[place], ("kv", "tp"), pairs))
        mixed = make_arranged(blocks, outs, ins, ranks, seq_local)
        return (mixed, root_state, next_value, next_write, next_read, step_out)
    stacked = jnp.concatenate(ys, axis=0)
    blocks = {}
    for step, chunks in zip(ins, columns):
        item = jnp.concatenate(chunks, axis=0)
        product = jnp.dot(stacked, item, preferred_element_type=jnp.float32)
        product = product.astype(jnp.bfloat16).reshape(len(outs), token_count, -1)
        for place, out in enumerate(outs):
            blocks[out ^ step] = swap(product[place], out) if out else product[place]
    blocks = jnp.stack([blocks[step] for step in range(ranks)])
    blocks = jnp.take(blocks, me ^ jnp.arange(ranks), axis=0)
    full = jnp.swapaxes(blocks, 0, 1).reshape(token_count, halves, width // halves)
    shares = lax.all_to_all(full, "tp", split_axis=1, concat_axis=1, tiled=True)
    mixed = jnp.sum(shares.astype(jnp.float32), axis=1).astype(jnp.bfloat16)
    mixed = mixed.reshape(seq_local, proposals, width // halves)
    return (mixed, root_state, next_value, next_write, next_read, step_out)


def solution(mesh):
    return jax.shard_map(
        whole_step,
        mesh=mesh,
        in_specs=(
            P("kv", None, "tp"),
            P(),
            P("kv", "tp"),
            P("kv", "tp"),
            P("kv", "tp"),
            P("kv", "tp"),
            P(),
            P(None, "tp"),
            P(None, "tp"),
            P(None, "tp"),
            P("tp"),
            P("tp"),
            P("tp"),
            P("tp"),
            P("tp", "kv"),
            P("kv", "tp", None, None),
            P("kv", None, "tp"),
            P("kv", None, "tp"),
            P("kv", None, "tp"),
            P("kv", None, "tp"),
            P("kv"),
        ),
        out_specs=(
            P("kv", None, "tp"),
            P("kv", "tp", None, None),
            P("kv", None, "tp"),
            P("kv", None, "tp"),
            P("kv", None, "tp"),
            P("kv", None, "tp"),
        ),
        check_vma=False,
    )
```
